32 devices in a mesh: sp: 2 (over x), tp: 16 (over z, y, core).
Axes of the slice: x: 2, y: 2, z: 4, core: 2. Of those that a mesh axis runs over, the one named last changes fastest.
Arguments:
- query_first: bfloat16 [1024, 1536], P('sp', 'tp'), may hold values from -10 to 10
- query_second: bfloat16 [1024, 2560], P('sp', 'tp'), may hold values from -10 to 10
- latent: bfloat16 [1024, 512], P('sp'), may hold values from -400 to 400
- key_rotary: bfloat16 [1024, 32], P('sp'), may hold values from -90 to 90
- latent_gain: float32 [512], replicated, may hold values from 0.1 to 1.9
- key_up_first: bfloat16 [512, 1024], P(None, 'tp'), may hold values from -0.25 to 0.25
- value_up_first: bfloat16 [512, 1024], P(None, 'tp'), may hold values from -0.25 to 0.25
- key_up_second: bfloat16 [512, 2048], P(None, 'tp'), may hold values from -0.25 to 0.25
- value_up_second: bfloat16 [512, 2048], P(None, 'tp'), may hold values from -0.25 to 0.25
- out_first: bfloat16 [1024, 2048], P('tp'), may hold values from -0.109375 to 0.109375
- out_second: bfloat16 [2048, 2048], P('tp'), may hold values from -0.109375 to 0.109375
- residual: bfloat16 [1024, 2048], P('sp'), may hold values from -16 to 16
- expert_gain: float32 [2048], replicated, may hold values from 0.1 to 1.9
- route_experts: int32 [1024, 2], P('sp'), may hold values from 0 to 31, all different within a row; in each aligned block of 32 rows (0 to 31, 32 to 63, ...) at most 3 rows name the same one
- route_scores: float32 [1024, 2], P('sp'), may hold values from -6 to 306
- gate_weight: bfloat16 [32, 2048, 4096], P('sp', None, 'tp'), may hold values from -0.375 to 0.375
- up_weight: bfloat16 [32, 2048, 4096], P('sp', None, 'tp'), may hold values from -0.375 to 0.375
- down_weight: bfloat16 [32, 4096, 2048], P('sp', 'tp'), may hold values from -0.013671875 to 0.013671875
Outputs:
- mixed: bfloat16 [1024, 2048], P(('sp', 'tp'))
The draws below stay inside these ranges and needn't reach their ends.
Inputs may be any that keep to these rules, and one draw needn't show every extreme that they name: `route_experts`: each row names 2 different experts. In every aligned block of 32 rows no expert is named more than 3 times, and in some blocks one is named exactly 3 times.
All inputs are finite; a program needn't handle non-finite values.
Results may differ from the reference program's by a relative error of at most 0.02.
The reference program's roundings to bfloat16 on the way count: a program that leaves them out, or rounds other values in their place, can miss the bound.
Values may be sent and summed in bfloat16 or wider, within the bound.
A program may use at most 128 MiB of HBM per device.

```python
import math
import jax
import jax.numpy as jnp
import numpy as np
from jax import lax

D = 2048
HA = 16
HB = 16
NA = 64
VA = 64
NB = 128
VB = 128
ROPE = 32
RANK = 512
FF = 4096
EXPERTS = 32
TOPK = 2
CAP = 3
TOK_SP = 512
TOKENS = 1024
N_SP = 2
N_TP = 16


def scaled_field(key, rows, columns, lower, upper):
    base_key, row_key, column_key = jax.random.split(key, 3)
    base = jnp.clip(jax.random.normal(base_key, (rows, columns), jnp.float32), -4.0, 4.0)
    row_scale = jnp.exp(jax.random.uniform(row_key, (rows, 1), jnp.float32, math.log(lower), math.log(upper)))
    column_scale = jnp.exp(jax.random.uniform(column_key, (1, columns), jnp.float32, math.log(lower), math.log(upper)))
    return base * row_scale * column_scale


def draw_latent(key, part):
    return scaled_field(jax.random.fold_in(key, 11), TOKENS, RANK, 1.0, 10.0).astype(jnp.bfloat16)


def draw_residual(key, part):
    return scaled_field(jax.random.fold_in(key, 12), TOKENS, D, 0.2, 2.0).astype(jnp.bfloat16)


def draw_key_rotary(key, part):
    base_key = jax.random.fold_in(jax.random.fold_in(key, 13), 0)
    base = jnp.clip(jax.random.normal(base_key, (TOKENS, ROPE), jnp.float32), -4.0, 4.0)
    return base.astype(jnp.bfloat16)


def draw_route_scores(key, part):
    base_key = jax.random.fold_in(jax.random.fold_in(key, 14), 0)
    base = jnp.clip(1.5 * jax.random.normal(base_key, (TOKENS, TOPK), jnp.float32), -6.0, 6.0)
    return base.astype(jnp.float32)


def levels(rng, dims, pieces, least, largest):
    def one(dim, shards_of):
        draws = jax.random.uniform(jax.random.fold_in(jax.random.fold_in(rng, 6), dim), (shards_of,), jnp.float32, least / len(pieces), largest / len(pieces))
        return jnp.repeat(jnp.exp(draws), dims[dim] // shards_of).reshape((-1,) + (1,) * (len(dims) - dim - 1))

    factor_of = one(*pieces[0])
    for cut in pieces[1:]:
        factor_of = factor_of * one(*cut)
    return factor_of


def routed_block(stream_key, own, number, rows, number_of, top, bound, lean):
    sequence = jax.random.permutation(stream_key, number_of)
    crowded, ordinary = portions_of(number_of, rows * top, bound, lean, True), portions_of(number_of, rows * top, bound, lean, False)
    places = jnp.arange(number_of)

    def named(lengths, rotation):
        used = int((lengths > 0).sum())
        fixed = max(1, used // 4)
        shifted = fixed + (places - fixed + rotation * (used - fixed)) % max(1, number_of - fixed)
        return jnp.zeros((number_of,), jnp.int32).at[sequence[jnp.where(places < fixed, places, shifted)]].set(jnp.asarray(lengths, jnp.int32))

    lengths = jnp.where(number % 4 == 0, named(crowded, number // 4), named(ordinary, number - number // 4 - 1))
    mixed = jax.random.permutation(jax.random.fold_in(own, 3), number_of)
    source_of, sink = mixed[0:number_of // 2 * 2:2], mixed[1:number_of // 2 * 2:2]
    margin = jnp.minimum(lengths[source_of] - 1, bound - lengths[sink]) // 2
    margin = jnp.where((source_of == sequence[0]) | (sink == sequence[0]) | (lengths[sink] == 0), 0, jnp.maximum(margin, 0))
    shifted = jax.random.randint(jax.random.fold_in(own, 4), (number_of // 2,), 0, 1 << 20) % (margin + 1)
    lengths = lengths.at[source_of].add(-shifted).at[sink].add(shifted)
    labels = jnp.searchsorted(jnp.cumsum(lengths), jnp.arange(rows * top), side="right").astype(jnp.int32)
    grid = labels.reshape(top, rows).T
    grid = grid[jax.random.permutation(jax.random.fold_in(own, 1), rows)]
    rotation = jax.random.randint(jax.random.fold_in(own, 2), (rows, 1), 0, top)
    return jnp.take_along_axis(grid, (jnp.arange(top)[None, :] + rotation) % top, axis=1)


def portions_of(amount, total, reach, skew, full):
    loads = [(1 << 20) // math.isqrt(grade ** skew) + 1 for grade in range(1, amount + 1)]
    largest = reach if full else min(reach, max(-(-total // amount), total * loads[0] // sum(loads)))
    least = 1 if total - largest >= amount - 1 else 0
    counts, surplus = [largest] + [least] * (amount - 1), total - largest - least * (amount - 1)
    while surplus > 0:
        free = [i for i in range(1, amount) if counts[i] < largest] or [i for i in range(1, amount) if counts[i] < reach]
        mass, budget = sum([loads[i] for i in free]), surplus
        for i in free:
            addition = min(reach - counts[i], max(1, budget * loads[i] // mass), surplus)
            counts[i] = counts[i] + addition
            surplus = surplus - addition
    return np.array(counts)


def scatter_about(key, dims, scale, limit, cuts=(), kind=jnp.bfloat16):
    array = scale * jax.random.normal(key, dims, jnp.float32)
    if cuts:
        array = array * levels(key, dims, cuts, -0.22, 0.18)
    return jnp.clip(array, -limit, limit).astype(kind)


def setup_inputs(seed: int = 0) -> dict:
    key_of = jax.random.split(jax.random.key(seed), 19)
    query_first = scatter_about(key_of[0], (TOKENS, HA * (NA + ROPE)), 2.5, 10.0, ((0, 2), (1, 16)))
    query_second = scatter_about(key_of[1], (TOKENS, HB * (NB + ROPE)), 2.5, 10.0, ((0, 2), (1, 16)))
    latent = draw_latent(jax.random.fold_in(key_of[18], 71), 0)
    key_rotary = draw_key_rotary(jax.random.fold_in(key_of[18], 71), 0)
    latent_gain = jnp.clip(1.0 + 0.18 * jax.random.normal(key_of[4], (RANK,), jnp.float32), 0.1, 1.9)
    key_up_first = scatter_about(key_of[5], (RANK, HA * NA), RANK ** -0.5, 0.25, ((1, 16),))
    value_up_first = scatter_about(key_of[6], (RANK, HA * VA), RANK ** -0.5, 0.25, ((1, 16),))
    key_up_second = scatter_about(key_of[7], (RANK, HB * NB), RANK ** -0.5, 0.25, ((1, 16),))
    value_up_second = scatter_about(key_of[8], (RANK, HB * VB), RANK ** -0.5, 0.25, ((1, 16),))
    out_first = scatter_about(key_of[9], (HA * VA, D), (HA * VA + HB * VB) ** -0.5, 0.109375, ((0, 16),))
    out_second = scatter_about(key_of[10], (HB * VB, D), (HA * VA + HB * VB) ** -0.5, 0.109375, ((0, 16),))
    residual = draw_residual(jax.random.fold_in(key_of[18], 71), 0)
    expert_gain = jnp.clip(1.0 + 0.18 * jax.random.normal(key_of[12], (D,), jnp.float32), 0.1, 1.9)
    route_experts_keys = jax.random.split(jax.random.fold_in(key_of[13], 1), TOKENS // (TOK_SP // N_TP))
    route_experts_turns = jax.random.permutation(jax.random.fold_in(key_of[13], 3), TOKENS // (TOK_SP // N_TP))
    route_experts = jax.vmap(lambda own, number: routed_block(jax.random.fold_in(key_of[13], 2), own, number, TOK_SP // N_TP, EXPERTS, TOPK, CAP, 2))(route_experts_keys, route_experts_turns).reshape((TOKENS, TOPK))
    route_scores = draw_route_scores(jax.random.fold_in(key_of[18], 71), 0)
    gate_weight = scatter_about(key_of[15], (EXPERTS, D, FF), (D // 9) ** -0.5, 0.375, ((0, 2), (2, 16)))
    up_weight = scatter_about(key_of[16], (EXPERTS, D, FF), (D // 9) ** -0.5, 0.375, ((0, 2), (2, 16)))
    down_weight = scatter_about(key_of[17], (EXPERTS, FF, D), (FF * 44) ** -0.5, 0.013671875, ((0, 2), (1, 16)))
    return {"query_first": query_first, "query_second": query_second, "latent": latent, "key_rotary": key_rotary, "latent_gain": latent_gain, "key_up_first": key_up_first, "value_up_first": value_up_first, "key_up_second": key_up_second, "value_up_second": value_up_second, "out_first": out_first, "out_second": out_second, "residual": residual, "expert_gain": expert_gain, "route_experts": route_experts, "route_scores": route_scores, "gate_weight": gate_weight, "up_weight": up_weight, "down_weight": down_weight}


norm_epsilon = 1e-06
rotary_base = 10000.0
clamp_limit = 7.0
sigmoid_slope = 1.702
masked_score = -1e+30

def rotate(values, positions):
    half = values.shape[-1] // 2
    inverse = rotary_base ** (-jnp.arange(half, dtype=jnp.float32) / half)
    angles = positions.astype(jnp.float32)[:, None, None] * inverse[None, None, :]
    cosine = jnp.cos(angles)
    sine = jnp.sin(angles)
    first = values[..., :half]
    second = values[..., half:]
    return jnp.concatenate([first * cosine - second * sine, second * cosine + first * sine], axis=-1)

def rms_scaled(values, gain):
    wide = values.astype(jnp.float32)
    return wide * lax.rsqrt(lax.optimization_barrier(jnp.mean(wide * wide, axis=-1, keepdims=True)) + norm_epsilon) * gain

def turned_queries(query, nope, positions):
    shaped = query.reshape(query.shape[0], query.shape[1] // (nope + ROPE), nope + ROPE)
    turned = rotate(shaped[..., nope:].astype(jnp.float32), positions).astype(jnp.bfloat16)
    return jnp.concatenate([shaped[..., :nope], turned], axis=-1)

def clamped_unit(gate, upward):
    limited = jnp.minimum(gate, clamp_limit)
    bounded = jnp.clip(upward, -clamp_limit, clamp_limit)
    return (bounded + 1.0) * limited * jax.nn.sigmoid(sigmoid_slope * limited)

def attend_group(queries, key_nope, key_turned, values, scale):
    total = queries.shape[0]
    step_rows = math.gcd(total, 512)
    heads = queries.shape[1]
    nope = key_nope.shape[1] // heads
    keys = key_nope.reshape(total, heads, nope).astype(jnp.float32)
    value_rows = values.reshape(total, heads, values.shape[1] // heads).astype(jnp.float32)
    turned = key_turned.astype(jnp.float32)
    key_places = jnp.arange(total, dtype=jnp.int32)

    def one_block(index):
        rows = lax.dynamic_slice_in_dim(queries, index * step_rows, step_rows, 0).astype(jnp.float32)
        score = jnp.einsum('qhd,khd->qhk', rows[..., :nope], keys)
        score = (score + jnp.einsum('qhr,kr->qhk', rows[..., nope:], turned)) * scale
        places = index * step_rows + jnp.arange(step_rows, dtype=jnp.int32)
        allowed = (places[:, None] >= key_places[None, :])[:, None, :]
        score = jnp.where(allowed, score, masked_score)
        highest = lax.optimization_barrier(jnp.max(score, axis=-1, keepdims=True))
        weights = jnp.where(allowed, jnp.exp(score - highest), 0.0)
        denominator = lax.optimization_barrier(jnp.sum(weights, axis=-1))
        rounded = lax.optimization_barrier(weights.astype(jnp.bfloat16)).astype(jnp.float32)
        numerator = jnp.einsum('qhk,khd->qhd', rounded, value_rows)
        return (numerator / denominator[..., None]).astype(jnp.bfloat16)
    blocks = lax.map(one_block, jnp.arange(total // step_rows, dtype=jnp.int32))
    return blocks.reshape(total, -1)

def reference(query_first, query_second, latent, key_rotary, latent_gain, key_up_first, value_up_first, key_up_second, value_up_second, out_first, out_second, residual, expert_gain, route_experts, route_scores, gate_weight, up_weight, down_weight):
    total = latent.shape[0]
    places = jnp.arange(total, dtype=jnp.int32)
    queries_first = turned_queries(query_first, NA, places)
    queries_second = turned_queries(query_second, NB, places)
    key_turned = rotate(key_rotary.astype(jnp.float32)[:, None, :], places)[:, 0, :].astype(jnp.bfloat16)
    latent_normed = rms_scaled(latent, latent_gain).astype(jnp.bfloat16)
    key_first = jnp.dot(latent_normed, key_up_first, preferred_element_type=jnp.float32).astype(jnp.bfloat16)
    key_second = jnp.dot(latent_normed, key_up_second, preferred_element_type=jnp.float32).astype(jnp.bfloat16)
    value_first = jnp.dot(latent_normed, value_up_first, preferred_element_type=jnp.float32).astype(jnp.bfloat16)
    value_second = jnp.dot(latent_normed, value_up_second, preferred_element_type=jnp.float32).astype(jnp.bfloat16)
    attended_first = attend_group(queries_first, key_first, key_turned, value_first, (NA + ROPE) ** (-0.5))
    attended_second = attend_group(queries_second, key_second, key_turned, value_second, (NB + ROPE) ** (-0.5))
    set_first = attended_first.shape[1] // N_TP
    set_second = attended_second.shape[1] // N_TP
    projected = jnp.zeros((total, residual.shape[1]), jnp.float32)
    for index in range(N_TP):
        partial_value = jnp.dot(attended_first[:, index * set_first:(index + 1) * set_first], out_first[index * set_first:(index + 1) * set_first], preferred_element_type=jnp.float32)
        partial_value = partial_value + jnp.dot(attended_second[:, index * set_second:(index + 1) * set_second], out_second[index * set_second:(index + 1) * set_second], preferred_element_type=jnp.float32)
        projected = projected + lax.optimization_barrier(partial_value.astype(jnp.bfloat16)).astype(jnp.float32)
    middle = (residual.astype(jnp.float32) + projected).astype(jnp.bfloat16)
    normed = rms_scaled(middle, expert_gain).astype(jnp.bfloat16)
    route_weight = jax.nn.softmax(route_scores, axis=-1)
    experts = gate_weight.shape[0]
    topk = route_experts.shape[1]
    block_rows = total // (N_SP * N_TP)
    blocks = total // block_rows
    chosen = route_experts.reshape(blocks, block_rows * topk)
    hits = (chosen[..., None] == jnp.arange(experts, dtype=jnp.int32)).astype(jnp.int32)
    ranks = lax.optimization_barrier(jnp.sum((jnp.cumsum(hits, axis=1) - hits) * hits, axis=-1))
    slot_place = jnp.arange(blocks, dtype=jnp.int32)[:, None] * CAP + ranks
    owners = jnp.broadcast_to(places.reshape(blocks, block_rows, 1), (blocks, block_rows, topk)).reshape(blocks, -1)
    table = jnp.full((experts, blocks * CAP), total, jnp.int32)
    table = table.at[chosen.reshape(-1), slot_place.reshape(-1)].set(owners.reshape(-1))
    padded = jnp.concatenate([normed, jnp.zeros((1, normed.shape[1]), jnp.bfloat16)], axis=0)

    def run_expert(operands):
        slots, gate_part, up_part, down_part = operands
        rows = padded[slots]
        gate = jnp.dot(rows, gate_part, preferred_element_type=jnp.float32)
        upward = jnp.dot(rows, up_part, preferred_element_type=jnp.float32)
        activated = clamped_unit(gate, upward).astype(jnp.bfloat16)
        unit_set = activated.shape[1] // N_TP
        parts = jnp.einsum('snf,nfd->snd', activated.reshape(-1, N_TP, unit_set).astype(jnp.float32), down_part.reshape(N_TP, unit_set, -1).astype(jnp.float32))
        rounded = lax.optimization_barrier(parts.astype(jnp.bfloat16)).astype(jnp.float32)
        return lax.optimization_barrier(jnp.sum(rounded, axis=1)).astype(jnp.bfloat16)
    results = lax.map(run_expert, (table, gate_weight, up_weight, down_weight))
    picked = results[chosen.reshape(-1), slot_place.reshape(-1)].reshape(total, topk, -1).astype(jnp.float32)
    mixture = lax.optimization_barrier(jnp.sum(route_weight[..., None] * picked, axis=1))
    return (middle.astype(jnp.float32) + mixture).astype(jnp.bfloat16)
```

```python
import functools

import jax
import jax.numpy as jnp
from jax import lax
from jax.experimental import pallas as pl
from jax.experimental.pallas import tpu as pltpu
from jax.sharding import PartitionSpec as P

NA = 64
NB = 128
ROPE = 32
CAP = 3


norm_epsilon = 1e-06
rotary_base = 10000.0
clamp_limit = 7.0
sigmoid_slope = 1.702
masked_score = -1e30


def rotate(values, positions):
    half = values.shape[-1] // 2
    inverse = rotary_base ** (-jnp.arange(half, dtype=jnp.float32) / half)
    angles = positions.astype(jnp.float32)[:, None, None] * inverse[None, None, :]
    cosine = jnp.cos(angles)
    sine = jnp.sin(angles)
    first = values[..., :half]
    second = values[..., half:]
    return jnp.concatenate(
        [first * cosine - second * sine, second * cosine + first * sine], axis=-1
    )


def rms_scaled(values, gain):
    wide = values.astype(jnp.float32)
    return wide * lax.rsqrt(jnp.mean(wide * wide, axis=-1, keepdims=True) + norm_epsilon) * gain


def turned_queries(query, nope, positions):
    shaped = query.reshape(query.shape[0], query.shape[1] // (nope + ROPE), nope + ROPE)
    turned = rotate(shaped[..., nope:].astype(jnp.float32), positions).astype(jnp.bfloat16)
    return jnp.concatenate([shaped[..., :nope], turned], axis=-1)


def clamped_unit(gate, upward):
    limited = jnp.minimum(gate, clamp_limit)
    bounded = jnp.clip(upward, -clamp_limit, clamp_limit)
    return (bounded + 1.0) * limited * jax.nn.sigmoid(sigmoid_slope * limited)


def slot_numbers(chosen, experts):
    hits = (chosen[..., None] == jnp.arange(experts, dtype=jnp.int32)).astype(jnp.int32)
    before = jnp.cumsum(hits, axis=-2) - hits
    return chosen * CAP + jnp.sum(before * hits, axis=-1)


def fold_group(state, queries, key_nope, key_turned, values, query_places, scale):
    running, denominator, numerator = state
    heads = queries.shape[1]
    nope = queries.shape[2] - key_turned.shape[1]
    keys = key_nope.reshape(key_nope.shape[0], heads, nope)
    value_rows = values.reshape(values.shape[0], heads, values.shape[1] // heads)
    score = jnp.einsum(
        "qhd,khd->qhk", queries[..., :nope], keys, preferred_element_type=jnp.float32
    )
    score = score + jnp.einsum(
        "qhr,kr->qhk", queries[..., nope:], key_turned, preferred_element_type=jnp.float32
    )
    score = score * scale
    key_places = jnp.arange(keys.shape[0], dtype=jnp.int32)
    allowed = (query_places[:, None] >= key_places[None, :])[:, None, :]
    score = jnp.where(allowed, score, masked_score)
    highest = jnp.maximum(running, jnp.max(score, axis=-1))
    weights = jnp.where(allowed, jnp.exp(score - highest[..., None]), 0.0)
    denominator = jnp.sum(weights, axis=-1)
    numerator = jnp.einsum(
        "qhk,khd->qhd", weights.astype(jnp.bfloat16), value_rows, preferred_element_type=jnp.float32
    )
    return (highest, denominator, numerator)


def expert_hidden(rows, gate_weight, up_weight):
    gate = jnp.einsum("nsecd,edf->nsecf", rows, gate_weight, preferred_element_type=jnp.float32)
    upward = jnp.einsum("nsecd,edf->nsecf", rows, up_weight, preferred_element_type=jnp.float32)
    return clamped_unit(gate, upward).astype(jnp.bfloat16)


def slot_body(
    query_first,
    query_second,
    latent,
    key_rotary,
    latent_gain,
    key_up_first,
    value_up_first,
    key_up_second,
    value_up_second,
    out_first,
    out_second,
    residual,
    expert_gain,
    route_experts,
    route_scores,
    gate_weight,
    up_weight,
    down_weight,
):
    seq_rows = latent.shape[0]
    sets = lax.axis_size("tp")
    groups = lax.axis_size("sp")
    own_rows = seq_rows // sets
    topk = route_experts.shape[1]
    local_experts = gate_weight.shape[0]
    experts = local_experts * groups
    offset = lax.axis_index("sp") * seq_rows
    places = offset + jnp.arange(seq_rows, dtype=jnp.int32)
    last_place = offset + seq_rows - 1
    queries_first = turned_queries(query_first, NA, places)
    queries_second = turned_queries(query_second, NB, places)
    key_turned = rotate(key_rotary.astype(jnp.float32)[:, None, :], places)[:, 0, :].astype(
        jnp.bfloat16
    )
    latent_normed = rms_scaled(latent, latent_gain).astype(jnp.bfloat16)
    scale_first = (NA + ROPE) ** (-0.5)
    scale_second = (NB + ROPE) ** (-0.5)

    def attend(carry, parts):
        key_first, value_first, key_second, value_second, turned = parts
        return (
            fold_group(
                carry[0], queries_first, key_first, turned, value_first, places, scale_first
            ),
            fold_group(
                carry[1], queries_second, key_second, turned, value_second, places, scale_second
            ),
        )

    def initial(queries, value_width):
        shape = queries.shape[:2]
        return (
            jnp.full(shape, masked_score, jnp.float32),
            jnp.zeros(shape, jnp.float32),
            jnp.zeros(shape + (value_width,), jnp.float32),
        )

    start_state = (
        initial(queries_first, value_up_first.shape[1] // queries_first.shape[1]),
        initial(queries_second, value_up_second.shape[1] // queries_second.shape[1]),
    )
    key_first, value_first, key_second, value_second = tuple(
        (
            jnp.dot(latent_normed, weight, preferred_element_type=jnp.float32).astype(jnp.bfloat16)
            for weight in (key_up_first, value_up_first, key_up_second, value_up_second)
        )
    )
    parts = (
        lax.all_gather(key_first, "sp", axis=0, tiled=True),
        lax.all_gather(value_first, "sp", axis=0, tiled=True),
        lax.all_gather(key_second, "sp", axis=0, tiled=True),
        lax.all_gather(value_second, "sp", axis=0, tiled=True),
        lax.all_gather(key_turned, "sp", axis=0, tiled=True),
    )
    state = lax.cond(
        jnp.int32(0) <= last_place,
        lambda inner: attend(inner, parts),
        lambda inner: inner,
        start_state,
    )
    first_state, second_state = state
    attended_first = (
        (first_state[2] / first_state[1][..., None]).astype(jnp.bfloat16).reshape(seq_rows, -1)
    )
    attended_second = (
        (second_state[2] / second_state[1][..., None]).astype(jnp.bfloat16).reshape(seq_rows, -1)
    )
    own_start = lax.axis_index("tp") * own_rows
    slot_range = jnp.arange(experts * CAP, dtype=jnp.int32)
    projected = lax.psum_scatter(
        (
            jnp.dot(attended_first, out_first, preferred_element_type=jnp.float32)
            + jnp.dot(attended_second, out_second, preferred_element_type=jnp.float32)
        ).astype(jnp.bfloat16),
        "tp",
        scatter_dimension=0,
        tiled=True,
    ).astype(jnp.float32)
    own_residual = lax.dynamic_slice_in_dim(residual, own_start, own_rows, 0)
    middle = (own_residual.astype(jnp.float32) + projected).astype(jnp.bfloat16)
    normed = rms_scaled(middle, expert_gain).astype(jnp.bfloat16)
    own_ids = lax.dynamic_slice_in_dim(route_experts, own_start, own_rows, 0).reshape(-1)
    own_slots = slot_numbers(own_ids, experts)
    picks = (own_slots[:, None] == slot_range).reshape(own_rows, topk, experts * CAP)
    selected = jnp.sum(picks.astype(jnp.float32), axis=1).astype(jnp.bfloat16)
    outgoing = jnp.einsum("ts,td->sd", selected, normed, preferred_element_type=jnp.float32).astype(
        jnp.bfloat16
    )
    outgoing = outgoing.reshape(groups, local_experts, CAP, outgoing.shape[-1])
    arrived = lax.all_to_all(outgoing, "sp", split_axis=0, concat_axis=0, tiled=True)
    activated = expert_hidden(
        lax.all_gather(arrived[None], "tp", axis=0, tiled=True), gate_weight, up_weight
    )
    flat_hidden = activated.reshape(sets * groups, local_experts, CAP, activated.shape[-1])
    summed = lax.psum_scatter(
        jnp.einsum(
            "secf,efd->secd", flat_hidden, down_weight, preferred_element_type=jnp.float32
        ).astype(jnp.bfloat16),
        "tp",
        scatter_dimension=0,
        tiled=True,
    )
    returned = lax.all_to_all(summed, "sp", split_axis=0, concat_axis=0, tiled=True)
    expert_out = returned.reshape(experts * CAP, returned.shape[-1]).astype(jnp.float32)
    own_scores = lax.dynamic_slice_in_dim(route_scores, own_start, own_rows, 0)
    route_weight = jax.nn.softmax(own_scores, axis=-1)
    matches = own_slots.reshape(own_rows, topk)[..., None] == slot_range
    combine = jnp.sum(jnp.where(matches, route_weight[..., None], 0.0), axis=1)
    mixture = jnp.dot(combine, expert_out, precision=lax.Precision.HIGHEST)
    return (middle.astype(jnp.float32) + mixture).astype(jnp.bfloat16)


MESH = pl.DeviceIdType.MESH
VMEM = pl.BlockSpec(memory_space=pltpu.VMEM)
TILE_TOKENS = 256
CHUNKS = 4


def places_of(axes):
    return {axis: lax.axis_index(axis) for axis in axes}


def bit_of(place, step):
    axis, mask = step
    return (place[axis] // mask) % 2


def partner_of(place, step):
    axis, mask = step
    return {axis: place[axis] + mask * (1 - 2 * bit_of(place, step))}


def greet(place, steps):
    barrier = pltpu.get_barrier_semaphore()
    for step in steps:
        pl.semaphore_signal(
            barrier, inc=1, device_id=partner_of(place, step), device_id_type=MESH
        )
    pl.semaphore_wait(barrier, len(steps))


def cube_steps(sp, tp):
    core = [("tp", 1)] if tp > 1 else []
    first = [("tp", 2)] if tp > 2 else []
    rest = [("tp", 1 << i) for i in range(2, tp.bit_length() - 1)]
    across = [("sp", 1 << i) for i in range(sp.bit_length() - 1)]
    return core, first, rest, across


def weight_of(step, widths):
    axis, mask = step
    return mask * (widths if axis == "sp" else 1)


def base_of(place, fixed, width):
    total = jnp.int32(0)
    for step in fixed:
        total = total + bit_of(place, step) * weight_of(step, width)
    return total


def offsets_of(free, width):
    found = [0]
    for step in free:
        found = found + [one + weight_of(step, width) for one in found]
    return found


def block_rows_of(index, rows):
    return pl.ds(pl.multiple_of(index * rows, rows), rows)


def scatter_kernel(
    orders, width, rows, x_ref, out_ref, total_ref, landing_ref, send_sem, recv_sem
):
    place = places_of(("sp", "tp"))
    stages = len(orders[0])
    cols = x_ref.shape[1] // len(orders)
    greet(place, orders[0])
    spots = [0]
    for number in range(stages):
        spots.append(spots[-1] + (1 << (stages - 1 - number)))

    def columns(part):
        return pl.ds(part * cols, cols)

    def start(part, number):
        order = orders[part]
        step = order[number]
        source = x_ref if number == 0 else total_ref
        base = base_of(place, order[:number], width)
        base = base + (1 - bit_of(place, step)) * weight_of(step, width)
        for slot, offset in enumerate(offsets_of(order[number + 1 :], width)):
            pltpu.make_async_remote_copy(
                src_ref=source.at[block_rows_of(base + offset, rows), columns(part)],
                dst_ref=landing_ref.at[pl.ds((spots[number] + slot) * rows, rows), columns(part)],
                send_sem=send_sem.at[part, number],
                recv_sem=recv_sem.at[part, number],
                device_id=partner_of(place, step),
                device_id_type=MESH,
            ).start()

    def drain(part, number, sem):
        count = 1 << (stages - 1 - number)
        whole = landing_ref.at[pl.ds(spots[number] * rows, count * rows), columns(part)]
        pltpu.make_async_copy(whole, whole, sem.at[part, number]).wait()

    def add(part, number):
        order = orders[part]
        source = x_ref if number == 0 else total_ref
        base = base_of(place, order[: number + 1], width)
        for slot, offset in enumerate(offsets_of(order[number + 1 :], width)):
            here = block_rows_of(base + offset, rows)
            there = pl.ds((spots[number] + slot) * rows, rows)
            value = source[here, columns(part)].astype(jnp.float32) + landing_ref[
                there, columns(part)
            ].astype(jnp.float32)
            if number + 1 < stages:
                total_ref[here, columns(part)] = value.astype(total_ref.dtype)
            else:
                out_ref[:, columns(part)] = value

    for part in range(len(orders)):
        start(part, 0)
    for wave in range(stages + 1):
        for part in range(len(orders)):
            number = wave - part // 2 % 2
            if number < 0 or number >= stages:
                continue
            drain(part, number, recv_sem)
            add(part, number)
            if number + 1 < stages:
                start(part, number + 1)
    for part in range(len(orders)):
        for number in range(stages):
            drain(part, number, send_sem)


def scatter_blocks(x, orders, width, count, collective_id):
    rows = x.shape[0] // count
    depth = x.shape[1]
    parts, stages = len(orders), len(orders[0])
    return pl.pallas_call(
        functools.partial(scatter_kernel, orders, width, rows),
        out_shape=jax.ShapeDtypeStruct((rows, depth), jnp.float32),
        in_specs=[VMEM],
        out_specs=VMEM,
        scratch_shapes=[
            pltpu.VMEM(x.shape, x.dtype),
            pltpu.VMEM(((count - 1) * rows, depth), x.dtype),
            pltpu.SemaphoreType.DMA((parts, stages)),
            pltpu.SemaphoreType.DMA((parts, stages)),
        ],
        compiler_params=pltpu.CompilerParams(
            collective_id=collective_id, has_side_effects=True, vmem_limit_bytes=16 << 20
        ),
        name="scatter_blocks",
    )(x)


def exchange_kernel(latent_ref, turn_ref, route_ref, l_out, t_out, r_out, send_sem, recv_sem, own_sem):
    place = places_of(("sp", "tp"))
    across, core = ("sp", 1), ("tp", 1)
    greet(place, (across, core))
    half = latent_ref.shape[0] // 2
    side = bit_of(place, core)
    me = place["sp"]
    other = 1 - me
    pairs = ((latent_ref, l_out), (turn_ref, t_out))
    mine = pl.ds(pl.multiple_of(side * half, half), half)
    crossing = []
    for number, (source, target) in enumerate(pairs):
        crossing.append(
            pltpu.make_async_remote_copy(
                src_ref=source.at[mine, :],
                dst_ref=target.at[me, mine, :],
                send_sem=send_sem.at[number],
                recv_sem=recv_sem.at[number],
                device_id=partner_of(place, across),
                device_id_type=MESH,
            )
        )
    crossing.append(
        pltpu.make_async_remote_copy(
            src_ref=route_ref,
            dst_ref=r_out.at[me],
            send_sem=send_sem.at[2],
            recv_sem=recv_sem.at[2],
            device_id=partner_of(place, across),
            device_id_type=MESH,
        )
    )
    for copy in crossing:
        copy.start()
    kept = [
        pltpu.make_async_copy(source, target.at[me], own_sem.at[number])
        for number, (source, target) in enumerate(pairs + ((route_ref, r_out),))
    ]
    for copy in kept:
        copy.start()
    passing = []
    for number, (source, target) in enumerate(pairs):
        crossing[number].wait_recv()
        spot = target.at[other, mine, :]
        copy = pltpu.make_async_remote_copy(
            src_ref=spot,
            dst_ref=spot,
            send_sem=send_sem.at[3 + number],
            recv_sem=recv_sem.at[3 + number],
            device_id=partner_of(place, core),
            device_id_type=MESH,
        )
        copy.start()
        passing.append(copy)
    crossing[2].wait_recv()
    for copy in crossing:
        copy.wait_send()
    for copy in kept + passing:
        copy.wait()


def exchange(latent, turn, route, collective_id):
    return pl.pallas_call(
        exchange_kernel,
        out_shape=tuple(
            jax.ShapeDtypeStruct((2,) + one.shape, one.dtype) for one in (latent, turn, route)
        ),
        in_specs=[VMEM] * 3,
        out_specs=(VMEM,) * 3,
        scratch_shapes=[
            pltpu.SemaphoreType.DMA((5,)),
            pltpu.SemaphoreType.DMA((5,)),
            pltpu.SemaphoreType.DMA((3,)),
        ],
        compiler_params=pltpu.CompilerParams(collective_id=collective_id, has_side_effects=True),
        name="exchange",
    )(latent, turn, route)


def flipped(value, mask, bits):
    total = 0
    for bit in range(bits):
        digit = (value // (1 << bit)) % 2
        total = total + (1 << bit) * (1 - digit if mask >> bit & 1 else digit)
    return total


def mixture_kernel(
    pitch,
    x_ref,
    middle_ref,
    code_ref,
    gate_ref,
    up_ref,
    down_ref,
    out_ref,
    tok,
    hot,
    hot_turned,
    scale,
    picked,
    gate_sum,
    up_sum,
    active,
    gate_buf,
    up_buf,
    down_buf,
    core_land,
    diag_land,
    side_land,
    line_land,
    own_sum,
    line_sem,
    side_sem,
    diag_sem,
    core_sem,
    pass_sem,
    core_back,
    diag_back,
    side_back,
    line_back,
    send_back,
    weight_sem,
    down_sem,
):
    groups, sets = lax.axis_size("sp"), lax.axis_size("tp")
    lines = sets // 4
    bits = lines.bit_length() - 1
    chunks, pairs, _, rows, width = tok.shape
    experts = picked.shape[0]
    tiles, span, tokens = hot.shape
    per_tile = tokens // (2 * rows)
    half = lines // 2
    sp, tp = lax.axis_index("sp"), lax.axis_index("tp")
    core, row, line = tp % 2, (tp // 2) % 2, tp // 4

    def device(side, at, up, half_chip):
        return {"sp": side, "tp": at * 4 + up * 2 + half_chip}

    def pair_of(side, at, up):
        return side * (sets // 2) + at * 2 + up

    at_line = [flipped(line, m, bits) for m in range(lines)]
    own = [pair_of(sp, at_line[m], row) for m in range(lines)]
    by_x = [pair_of(1 - sp, at_line[m], row) for m in range(lines)]
    by_y = [pair_of(sp, at_line[m], 1 - row) for m in range(lines)]
    by_xy = [pair_of(1 - sp, at_line[m], 1 - row) for m in range(lines)]
    x_device = device(1 - sp, line, row, core)
    y_device = device(sp, line, 1 - row, core)
    core_device = device(sp, line, row, 1 - core)
    line_device = [device(sp, at_line[m], row, core) for m in range(lines)]

    barrier = pltpu.get_barrier_semaphore()
    everyone = [x_device, y_device, core_device] + line_device[1:]
    for one in everyone:
        pl.semaphore_signal(barrier, inc=1, device_id=one, device_id_type=MESH)

    def weight_copies(chunk):
        part = pl.ds(chunk * width, width)
        slot = chunk % 2
        return (
            pltpu.make_async_copy(
                gate_ref.at[:, part, :], gate_buf.at[slot], weight_sem.at[slot, 0]
            ),
            pltpu.make_async_copy(up_ref.at[:, part, :], up_buf.at[slot], weight_sem.at[slot, 1]),
        )

    def down_copy(chunk):
        part = pl.ds(chunk * width, width)
        return pltpu.make_async_copy(
            down_ref.at[:, :, part], down_buf.at[chunk], down_sem.at[chunk]
        )

    for chunk in range(min(2, chunks)):
        for copy in weight_copies(chunk):
            copy.start()

    pl.semaphore_wait(barrier, len(everyone))

    def push(source, target, send, receive, where):
        pltpu.make_async_remote_copy(
            src_ref=source,
            dst_ref=target,
            send_sem=send,
            recv_sem=receive,
            device_id=where,
            device_id_type=MESH,
        ).start()

    def settle(view, sem):
        pltpu.make_async_copy(view, view, sem).wait()

    def spot(chunk, pair):
        return tok.at[chunk, pair, core]

    def share(chunk, pair, part):
        push(
            spot(chunk, pair),
            spot(chunk, pair),
            pass_sem.at[chunk, part],
            core_sem.at[chunk],
            core_device,
        )

    def send_own(chunk):
        source = x_ref.at[:, pl.ds(chunk * width, width)]
        target = spot(chunk, own[0])
        early = pass_sem.at[chunk, 0]
        for m in range(1, lines):
            push(source, target, early, line_sem.at[chunk, m - 1], line_device[m])
        push(source, target, early, side_sem.at[chunk, 0, 0], x_device)
        push(source, target, early, side_sem.at[chunk, 1, 0], y_device)
        push(source, target, early, core_sem.at[chunk], core_device)

    def pass_line(chunk):
        for m in range(1, lines):
            settle(spot(chunk, own[m]), line_sem.at[chunk, m - 1])
            here = spot(chunk, own[m])
            early = pass_sem.at[chunk, 0]
            push(here, here, early, side_sem.at[chunk, 0, m], x_device)
            push(here, here, early, side_sem.at[chunk, 1, m], y_device)
            share(chunk, own[m], 0)

    def pass_side(chunk):
        for m in [*range(half, lines), *range(half)]:
            turn = ((0, by_x), (1, by_y)) if m >= half else ((1, by_y), (0, by_x))
            for axis, column in turn:
                here = spot(chunk, column[m])
                settle(here, side_sem.at[chunk, axis, m])
                late = pass_sem.at[chunk, 1]
                if axis == 0 and m >= half:
                    push(here, here, late, diag_sem.at[chunk, m], y_device)
                if axis == 1 and m < half:
                    push(here, here, late, diag_sem.at[chunk, m], x_device)
                share(chunk, column[m], 1)

    def pass_diag(chunk):
        for m in range(lines):
            settle(spot(chunk, by_xy[m]), diag_sem.at[chunk, m])
            share(chunk, by_xy[m], 1)

    def finish(chunk):
        settle(tok.at[chunk, :, 0], core_sem.at[chunk])

    for chunk in range(chunks):
        send_own(chunk)
    for chunk in range(chunks):
        tok[chunk, own[0], core] = x_ref[:, chunk * width : (chunk + 1) * width]

    for tile in range(tiles):
        slots = lax.broadcasted_iota(jnp.int32, (span, tokens), 0)
        first = slots == code_ref[tile, pl.ds(0, 1), :].astype(jnp.int32)
        second = slots == code_ref[tile, pl.ds(1, 1), :].astype(jnp.int32)
        chosen = jnp.where(first | second, 1.0, 0.0)
        hot[tile] = chosen.astype(jnp.bfloat16)
        hot_turned[tile] = chosen.T.astype(jnp.bfloat16)
        portion = jnp.where(first, code_ref[tile, pl.ds(2, 1), :], 0.0) + jnp.where(
            second, code_ref[tile, pl.ds(3, 1), :], 0.0
        )
        scale[:, tile * pitch : (tile + 1) * pitch, :] = jnp.sum(
            portion, axis=1, keepdims=True
        ).reshape(experts, pitch, 1)

    def pick(chunk, tile):
        block = tok[chunk, tile * per_tile : (tile + 1) * per_tile].reshape(tokens, width)
        found = jnp.dot(hot[tile], block, preferred_element_type=jnp.float32)
        picked[:, tile * pitch : (tile + 1) * pitch, :] = found.astype(jnp.bfloat16).reshape(
            experts, pitch, width
        )

    def hidden(chunk, low, high):
        slot = chunk % 2

        def one(expert, carry):
            block = picked[expert]
            gate = jnp.dot(block, gate_buf[slot, expert], preferred_element_type=jnp.float32)
            upward = jnp.dot(block, up_buf[slot, expert], preferred_element_type=jnp.float32)
            if chunk > 0:
                gate = gate + gate_sum[expert]
                upward = upward + up_sum[expert]
            if chunk + 1 < chunks:
                gate_sum[expert] = gate
                up_sum[expert] = upward
            else:
                active[expert] = clamped_unit(gate, upward).astype(jnp.bfloat16)
            return carry

        lax.fori_loop(low, high, one, 0, unroll=2)

    pass_line(0)
    if chunks > 1:
        pass_line(1)
    pass_side(0)
    if chunks > 2:
        pass_line(2)
    pass_diag(0)
    for chunk in range(chunks):
        finish(chunk)
        for tile in range(tiles):
            pick(chunk, tile)
        if chunk + 1 < chunks:
            pass_side(chunk + 1)
        for copy in weight_copies(chunk):
            copy.wait()
        hidden(chunk, 0, experts // 2)
        if chunk + 3 < chunks:
            pass_line(chunk + 3)
        if chunk + 1 < chunks:
            pass_diag(chunk + 1)
        hidden(chunk, experts // 2, experts)
        if chunk + 2 < chunks:
            for copy in weight_copies(chunk + 2):
                copy.start()
        if chunk == 0:
            for later in range(chunks):
                down_copy(later).start()

    for chunk in range(chunks):
        settle(tok.at[chunk, : pairs - 1, 0], pass_sem.at[chunk, 0])
        settle(tok.at[chunk, :, 0], pass_sem.at[chunk, 1])

    def lower(chunk):
        down_copy(chunk).wait()

        def one(expert, carry):
            result = jnp.dot(
                active[expert], down_buf[chunk, expert], preferred_element_type=jnp.float32
            )
            picked[expert] = (result * scale[expert]).astype(jnp.bfloat16)
            return carry

        lax.fori_loop(0, experts, one, 0, unroll=2)
        for tile in range(tiles):
            block = picked[:, tile * pitch : (tile + 1) * pitch, :].reshape(span, width)
            total = jnp.dot(hot_turned[tile], block, preferred_element_type=jnp.float32)
            tok[chunk, tile * per_tile : (tile + 1) * per_tile] = total.astype(
                jnp.bfloat16
            ).reshape(per_tile, 2, rows, width)

    def meet_core(chunk):
        push(
            tok.at[chunk, :, 1 - core],
            core_land.at[chunk],
            send_back.at[chunk, 0],
            core_back.at[chunk],
            core_device,
        )

    def add_core(chunk, pair):
        tok[chunk, pair, core] = (
            tok[chunk, pair, core].astype(jnp.float32) + core_land[chunk, pair].astype(jnp.float32)
        ).astype(jnp.bfloat16)

    def back_diag(chunk):
        settle(core_land.at[chunk], core_back.at[chunk])
        send = send_back.at[chunk, 1]
        for m in range(lines):
            add_core(chunk, by_xy[m])
            push(
                spot(chunk, by_xy[m]),
                diag_land.at[chunk, m],
                send,
                diag_back.at[chunk, m],
                y_device if m >= half else x_device,
            )
        for m in range(lines):
            axis, column, where = (1, by_y, y_device) if m >= half else (0, by_x, x_device)
            add_core(chunk, column[m])
            push(
                spot(chunk, column[m]),
                side_land.at[chunk, axis, m],
                send,
                side_back.at[chunk, axis, m],
                where,
            )
        for m in range(lines):
            add_core(chunk, (by_x if m >= half else by_y)[m])
            add_core(chunk, own[m])

    def back_side(chunk):
        for m in range(lines):
            axis, column, where = (0, by_x, x_device) if m >= half else (1, by_y, y_device)
            settle(diag_land.at[chunk, m], diag_back.at[chunk, m])
            tok[chunk, column[m], core] = (
                tok[chunk, column[m], core].astype(jnp.float32)
                + diag_land[chunk, m].astype(jnp.float32)
            ).astype(jnp.bfloat16)
            push(
                spot(chunk, column[m]),
                side_land.at[chunk, axis, m],
                send_back.at[chunk, 2],
                side_back.at[chunk, axis, m],
                where,
            )

    def back_line(chunk):
        for m in [*range(1, lines), 0]:
            total = tok[chunk, own[m], core].astype(jnp.float32)
            for axis in range(2):
                settle(side_land.at[chunk, axis, m], side_back.at[chunk, axis, m])
                total = total + side_land[chunk, axis, m].astype(jnp.float32)
            if m == 0:
                own_sum[chunk] = total
                continue
            tok[chunk, own[m], core] = total.astype(jnp.bfloat16)
            push(
                spot(chunk, own[m]),
                line_land.at[chunk, m - 1],
                send_back.at[chunk, 3],
                line_back.at[chunk, m - 1],
                line_device[m],
            )

    def close(chunk):
        total = own_sum[chunk]
        for m in range(1, lines):
            settle(line_land.at[chunk, m - 1], line_back.at[chunk, m - 1])
            total = total + line_land[chunk, m - 1].astype(jnp.float32)
        part = slice(chunk * width, (chunk + 1) * width)
        out_ref[:, part] = (middle_ref[:, part].astype(jnp.float32) + total).astype(jnp.bfloat16)

    stages = (back_diag, back_side, back_line, close)
    for step in range(chunks + len(stages)):
        if step < chunks:
            lower(step)
            meet_core(step)
        for number, stage in enumerate(stages):
            chunk = step - 1 - number
            if 0 <= chunk < chunks:
                stage(chunk)
    for chunk in range(chunks):
        settle(core_land.at[chunk], send_back.at[chunk, 0])
        settle(tok.at[chunk, : 2 * lines, 0], send_back.at[chunk, 1])
        settle(tok.at[chunk, :lines, 0], send_back.at[chunk, 2])
        settle(tok.at[chunk, : lines - 1, 0], send_back.at[chunk, 3])


def run_mixture(
    tokens, middle, codes, gate_weight, up_weight, down_weight, pitch, chunks, collective_id
):
    experts, depth, units = gate_weight.shape
    tiles, _, tile_tokens = codes.shape
    rows = tokens.shape[0]
    groups, sets = lax.axis_size("sp"), lax.axis_size("tp")
    pairs, lines = groups * sets // 2, sets // 4
    width = depth // chunks
    span = experts * pitch
    narrow, wide = jnp.bfloat16, jnp.float32
    anywhere = pl.BlockSpec(memory_space=pl.ANY)
    dma = pltpu.SemaphoreType.DMA
    return pl.pallas_call(
        functools.partial(mixture_kernel, pitch),
        out_shape=jax.ShapeDtypeStruct(tokens.shape, jnp.bfloat16),
        in_specs=[VMEM, VMEM, VMEM, anywhere, anywhere, anywhere],
        out_specs=VMEM,
        scratch_shapes=[
            pltpu.VMEM((chunks, pairs, 2, rows, width), narrow),
            pltpu.VMEM((tiles, span, tile_tokens), narrow),
            pltpu.VMEM((tiles, tile_tokens, span), narrow),
            pltpu.VMEM((experts, tiles * pitch, 1), wide),
            pltpu.VMEM((experts, tiles * pitch, width), narrow),
            pltpu.VMEM((experts, tiles * pitch, units), wide),
            pltpu.VMEM((experts, tiles * pitch, units), wide),
            pltpu.VMEM((experts, tiles * pitch, units), narrow),
            pltpu.VMEM((2, experts, width, units), narrow),
            pltpu.VMEM((2, experts, width, units), narrow),
            pltpu.VMEM((chunks, experts, units, width), narrow),
            pltpu.VMEM((chunks, pairs, rows, width), narrow),
            pltpu.VMEM((chunks, lines, rows, width), narrow),
            pltpu.VMEM((chunks, 2, lines, rows, width), narrow),
            pltpu.VMEM((chunks, lines - 1, rows, width), narrow),
            pltpu.VMEM((chunks, rows, width), wide),
            dma((chunks, lines - 1)),
            dma((chunks, 2, lines)),
            dma((chunks, lines)),
            dma((chunks,)),
            dma((chunks, 2)),
            dma((chunks,)),
            dma((chunks, lines)),
            dma((chunks, 2, lines)),
            dma((chunks, lines - 1)),
            dma((chunks, 4)),
            dma((2, 2)),
            dma((chunks,)),
        ],
        compiler_params=pltpu.CompilerParams(
            collective_id=collective_id, has_side_effects=True, vmem_limit_bytes=63 << 20
        ),
        name="run_mixture",
    )(tokens, middle, codes, gate_weight, up_weight, down_weight)


def attended_heads(queries, nope, keys, turned, values, allowed, scale):
    heads = queries.shape[1]
    wide = keys.reshape(keys.shape[0], heads, nope)
    shared = jnp.broadcast_to(turned[:, None, :], (turned.shape[0], heads, turned.shape[1]))
    whole = jnp.concatenate([wide, shared], axis=-1)
    value_rows = values.reshape(values.shape[0], heads, values.shape[1] // heads)
    score = jnp.einsum("qhd,khd->hqk", queries, whole, preferred_element_type=jnp.float32) * scale
    score = jnp.where(allowed, score, masked_score)
    highest = jnp.max(score, axis=-1, keepdims=True)
    weights = jnp.exp(score - highest)
    denominator = jnp.sum(weights, axis=-1)
    numerator = jnp.einsum(
        "hqk,khd->hqd", weights.astype(jnp.bfloat16), value_rows, preferred_element_type=jnp.float32
    )
    attended = (numerator / denominator[..., None]).astype(jnp.bfloat16)
    return jnp.swapaxes(attended, 0, 1).reshape(attended.shape[1], -1)


def token_body(
    query_first,
    query_second,
    latent,
    key_rotary,
    latent_gain,
    key_up_first,
    value_up_first,
    key_up_second,
    value_up_second,
    out_first,
    out_second,
    residual,
    expert_gain,
    route_experts,
    route_scores,
    gate_weight,
    up_weight,
    down_weight,
):
    seq_rows = latent.shape[0]
    sets = lax.axis_size("tp")
    groups = lax.axis_size("sp")
    own_rows = seq_rows // sets
    local_experts = gate_weight.shape[0]
    total = groups * seq_rows
    me = lax.axis_index("sp")
    core, first, rest, across = cube_steps(groups, sets)
    span_blocks = TILE_TOKENS // own_rows
    pitch = -(-span_blocks * CAP // 16) * 16

    chosen = route_experts.reshape(sets, -1)
    earlier = jnp.tril(jnp.ones((chosen.shape[1],) * 2, jnp.float32), -1)
    same = (chosen[:, :, None] == chosen[:, None, :]).astype(jnp.float32)
    rank = jnp.sum(same * earlier, axis=-1)
    spot = ((jnp.arange(sets, dtype=jnp.int32) % span_blocks) * CAP).astype(jnp.float32)
    code = chosen.astype(jnp.float32) * pitch + spot[:, None] + rank
    code = code.reshape(seq_rows, -1).T
    scores = route_scores.T
    raised = jnp.exp(scores - jnp.max(scores, axis=0, keepdims=True))
    share = raised / jnp.sum(raised, axis=0, keepdims=True)
    route = jnp.concatenate([code, share, code, share], axis=0)

    rotary = key_rotary.shape[1]
    wide_rotary = jnp.pad(key_rotary, ((0, 0), (0, -rotary % 128)))
    latents, turns, routes = exchange(latent, wide_rotary, route, 0)

    places = me * seq_rows + jnp.arange(seq_rows, dtype=jnp.int32)
    all_places = jnp.arange(total, dtype=jnp.int32)
    queries_first = turned_queries(query_first, NA, places)
    queries_second = turned_queries(query_second, NB, places)
    turned = rotate(
        turns.reshape(total, -1)[:, :rotary].astype(jnp.float32)[:, None, :], all_places
    )[:, 0, :].astype(jnp.bfloat16)
    latent_normed = rms_scaled(latents.reshape(total, -1), latent_gain).astype(jnp.bfloat16)
    key_first, value_first, key_second, value_second = tuple(
        jnp.dot(latent_normed, weight, preferred_element_type=jnp.float32).astype(jnp.bfloat16)
        for weight in (key_up_first, value_up_first, key_up_second, value_up_second)
    )
    allowed = (places[:, None] >= all_places[None, :])[None]
    attended_first = attended_heads(
        queries_first, NA, key_first, turned, value_first, allowed, (NA + ROPE) ** (-0.5)
    )
    attended_second = attended_heads(
        queries_second, NB, key_second, turned, value_second, allowed, (NB + ROPE) ** (-0.5)
    )
    partial = (
        jnp.dot(attended_first, out_first, preferred_element_type=jnp.float32)
        + jnp.dot(attended_second, out_second, preferred_element_type=jnp.float32)
    ).astype(jnp.bfloat16)
    one, two = tuple(core + first + rest), tuple(core + rest + first)
    projected = scatter_blocks(partial, (one, two, one, one), sets, sets, 1)
    own_start = lax.axis_index("tp") * own_rows
    own_residual = lax.dynamic_slice_in_dim(residual, own_start, own_rows, 0)
    middle = (own_residual.astype(jnp.float32) + projected).astype(jnp.bfloat16)
    normed = rms_scaled(middle, expert_gain).astype(jnp.bfloat16)
    tiles = total // TILE_TOKENS
    codes = jnp.swapaxes(routes, 0, 1).reshape(8, total)
    shift = jnp.array([1.0, 1.0, 0.0, 0.0, 1.0, 1.0, 0.0, 0.0], jnp.float32)
    codes = codes - (shift * (me * local_experts * pitch).astype(jnp.float32))[:, None]
    codes = jnp.swapaxes(codes.reshape(8, tiles, TILE_TOKENS), 0, 1)
    return run_mixture(
        normed, middle, codes, gate_weight, up_weight, down_weight, pitch, CHUNKS, 2
    )


def solution(mesh):
    in_specs = (
        P("sp", "tp"),
        P("sp", "tp"),
        P("sp", None),
        P("sp", None),
        P(),
        P(None, "tp"),
        P(None, "tp"),
        P(None, "tp"),
        P(None, "tp"),
        P("tp", None),
        P("tp", None),
        P("sp", None),
        P(),
        P("sp", None),
        P("sp", None),
        P("sp", None, "tp"),
        P("sp", None, "tp"),
        P("sp", "tp", None),
    )
    out_specs = P(("sp", "tp"), None)
    groups, sets = mesh.shape["sp"], mesh.shape["tp"]
    small = groups == 2 and sets & (sets - 1) == 0 and sets > 4

    def body(*arguments):
        fits = small and arguments[2].shape[0] * groups <= 1024
        return (token_body if fits else slot_body)(*arguments)

    return jax.shard_map(body, mesh=mesh, in_specs=in_specs, out_specs=out_specs, check_vma=False)
```

```python
import functools

import jax
import jax.numpy as jnp
import numpy as np
from jax import lax
from jax.experimental import pallas as pl
from jax.experimental.pallas import tpu as pltpu
from jax.sharding import PartitionSpec as P

NA = 64
NB = 128
ROPE = 32
CAP = 3


norm_epsilon = 1e-06
rotary_base = 10000.0
clamp_limit = 7.0
sigmoid_slope = 1.702
masked_score = -1e30


def rotate(values, positions):
    half = values.shape[-1] // 2
    inverse = rotary_base ** (-jnp.arange(half, dtype=jnp.float32) / half)
    angles = positions.astype(jnp.float32)[:, None, None] * inverse[None, None, :]
    cosine = jnp.cos(angles)
    sine = jnp.sin(angles)
    first = values[..., :half]
    second = values[..., half:]
    return jnp.concatenate(
        [first * cosine - second * sine, second * cosine + first * sine], axis=-1
    )


def rms_scaled(values, gain):
    wide = values.astype(jnp.float32)
    return wide * lax.rsqrt(jnp.mean(wide * wide, axis=-1, keepdims=True) + norm_epsilon) * gain


def turned_queries(query, nope, positions):
    shaped = query.reshape(query.shape[0], query.shape[1] // (nope + ROPE), nope + ROPE)
    turned = rotate(shaped[..., nope:].astype(jnp.float32), positions).astype(jnp.bfloat16)
    return jnp.concatenate([shaped[..., :nope], turned], axis=-1)


def clamped_unit(gate, upward):
    limited = jnp.minimum(gate, clamp_limit)
    bounded = jnp.clip(upward, -clamp_limit, clamp_limit)
    return (bounded + 1.0) * limited * jax.nn.sigmoid(sigmoid_slope * limited)


def slot_numbers(chosen, experts):
    hits = (chosen[..., None] == jnp.arange(experts, dtype=jnp.int32)).astype(jnp.int32)
    before = jnp.cumsum(hits, axis=-2) - hits
    return chosen * CAP + jnp.sum(before * hits, axis=-1)


def fold_group(state, queries, key_nope, key_turned, values, query_places, scale):
    running, denominator, numerator = state
    heads = queries.shape[1]
    nope = queries.shape[2] - key_turned.shape[1]
    keys = key_nope.reshape(key_nope.shape[0], heads, nope)
    value_rows = values.reshape(values.shape[0], heads, values.shape[1] // heads)
    score = jnp.einsum(
        "qhd,khd->qhk", queries[..., :nope], keys, preferred_element_type=jnp.float32
    )
    score = score + jnp.einsum(
        "qhr,kr->qhk", queries[..., nope:], key_turned, preferred_element_type=jnp.float32
    )
    score = score * scale
    key_places = jnp.arange(keys.shape[0], dtype=jnp.int32)
    allowed = (query_places[:, None] >= key_places[None, :])[:, None, :]
    score = jnp.where(allowed, score, masked_score)
    highest = jnp.maximum(running, jnp.max(score, axis=-1))
    weights = jnp.where(allowed, jnp.exp(score - highest[..., None]), 0.0)
    denominator = jnp.sum(weights, axis=-1)
    numerator = jnp.einsum(
        "qhk,khd->qhd", weights.astype(jnp.bfloat16), value_rows, preferred_element_type=jnp.float32
    )
    return (highest, denominator, numerator)


def expert_hidden(rows, gate_weight, up_weight):
    gate = jnp.einsum("nsecd,edf->nsecf", rows, gate_weight, preferred_element_type=jnp.float32)
    upward = jnp.einsum("nsecd,edf->nsecf", rows, up_weight, preferred_element_type=jnp.float32)
    return clamped_unit(gate, upward).astype(jnp.bfloat16)


def slot_body(
    query_first,
    query_second,
    latent,
    key_rotary,
    latent_gain,
    key_up_first,
    value_up_first,
    key_up_second,
    value_up_second,
    out_first,
    out_second,
    residual,
    expert_gain,
    route_experts,
    route_scores,
    gate_weight,
    up_weight,
    down_weight,
):
    seq_rows = latent.shape[0]
    sets = lax.axis_size("tp")
    groups = lax.axis_size("sp")
    own_rows = seq_rows // sets
    topk = route_experts.shape[1]
    local_experts = gate_weight.shape[0]
    experts = local_experts * groups
    offset = lax.axis_index("sp") * seq_rows
    places = offset + jnp.arange(seq_rows, dtype=jnp.int32)
    last_place = offset + seq_rows - 1
    queries_first = turned_queries(query_first, NA, places)
    queries_second = turned_queries(query_second, NB, places)
    key_turned = rotate(key_rotary.astype(jnp.float32)[:, None, :], places)[:, 0, :].astype(
        jnp.bfloat16
    )
    latent_normed = rms_scaled(latent, latent_gain).astype(jnp.bfloat16)
    scale_first = (NA + ROPE) ** (-0.5)
    scale_second = (NB + ROPE) ** (-0.5)

    def attend(carry, parts):
        key_first, value_first, key_second, value_second, turned = parts
        return (
            fold_group(
                carry[0], queries_first, key_first, turned, value_first, places, scale_first
            ),
            fold_group(
                carry[1], queries_second, key_second, turned, value_second, places, scale_second
            ),
        )

    def initial(queries, value_width):
        shape = queries.shape[:2]
        return (
            jnp.full(shape, masked_score, jnp.float32),
            jnp.zeros(shape, jnp.float32),
            jnp.zeros(shape + (value_width,), jnp.float32),
        )

    start_state = (
        initial(queries_first, value_up_first.shape[1] // queries_first.shape[1]),
        initial(queries_second, value_up_second.shape[1] // queries_second.shape[1]),
    )
    key_first, value_first, key_second, value_second = tuple(
        (
            jnp.dot(latent_normed, weight, preferred_element_type=jnp.float32).astype(jnp.bfloat16)
            for weight in (key_up_first, value_up_first, key_up_second, value_up_second)
        )
    )
    parts = (
        lax.all_gather(key_first, "sp", axis=0, tiled=True),
        lax.all_gather(value_first, "sp", axis=0, tiled=True),
        lax.all_gather(key_second, "sp", axis=0, tiled=True),
        lax.all_gather(value_second, "sp", axis=0, tiled=True),
        lax.all_gather(key_turned, "sp", axis=0, tiled=True),
    )
    state = lax.cond(
        jnp.int32(0) <= last_place,
        lambda inner: attend(inner, parts),
        lambda inner: inner,
        start_state,
    )
    first_state, second_state = state
    attended_first = (
        (first_state[2] / first_state[1][..., None]).astype(jnp.bfloat16).reshape(seq_rows, -1)
    )
    attended_second = (
        (second_state[2] / second_state[1][..., None]).astype(jnp.bfloat16).reshape(seq_rows, -1)
    )
    own_start = lax.axis_index("tp") * own_rows
    slot_range = jnp.arange(experts * CAP, dtype=jnp.int32)
    projected = lax.psum_scatter(
        (
            jnp.dot(attended_first, out_first, preferred_element_type=jnp.float32)
            + jnp.dot(attended_second, out_second, preferred_element_type=jnp.float32)
        ).astype(jnp.bfloat16),
        "tp",
        scatter_dimension=0,
        tiled=True,
    ).astype(jnp.float32)
    own_residual = lax.dynamic_slice_in_dim(residual, own_start, own_rows, 0)
    middle = (own_residual.astype(jnp.float32) + projected).astype(jnp.bfloat16)
    normed = rms_scaled(middle, expert_gain).astype(jnp.bfloat16)
    own_ids = lax.dynamic_slice_in_dim(route_experts, own_start, own_rows, 0).reshape(-1)
    own_slots = slot_numbers(own_ids, experts)
    picks = (own_slots[:, None] == slot_range).reshape(own_rows, topk, experts * CAP)
    selected = jnp.sum(picks.astype(jnp.float32), axis=1).astype(jnp.bfloat16)
    outgoing = jnp.einsum("ts,td->sd", selected, normed, preferred_element_type=jnp.float32).astype(
        jnp.bfloat16
    )
    outgoing = outgoing.reshape(groups, local_experts, CAP, outgoing.shape[-1])
    arrived = lax.all_to_all(outgoing, "sp", split_axis=0, concat_axis=0, tiled=True)
    activated = expert_hidden(
        lax.all_gather(arrived[None], "tp", axis=0, tiled=True), gate_weight, up_weight
    )
    flat_hidden = activated.reshape(sets * groups, local_experts, CAP, activated.shape[-1])
    summed = lax.psum_scatter(
        jnp.einsum(
            "secf,efd->secd", flat_hidden, down_weight, preferred_element_type=jnp.float32
        ).astype(jnp.bfloat16),
        "tp",
        scatter_dimension=0,
        tiled=True,
    )
    returned = lax.all_to_all(summed, "sp", split_axis=0, concat_axis=0, tiled=True)
    expert_out = returned.reshape(experts * CAP, returned.shape[-1]).astype(jnp.float32)
    own_scores = lax.dynamic_slice_in_dim(route_scores, own_start, own_rows, 0)
    route_weight = jax.nn.softmax(own_scores, axis=-1)
    matches = own_slots.reshape(own_rows, topk)[..., None] == slot_range
    combine = jnp.sum(jnp.where(matches, route_weight[..., None], 0.0), axis=1)
    mixture = jnp.dot(combine, expert_out, precision=lax.Precision.HIGHEST)
    return (middle.astype(jnp.float32) + mixture).astype(jnp.bfloat16)


MESH = pl.DeviceIdType.MESH
VMEM = pl.BlockSpec(memory_space=pltpu.VMEM)
TILE_TOKENS = 256
CHUNKS = 4


def flipped(value, mask, bits):
    total = 0
    for bit in range(bits):
        digit = (value // (1 << bit)) % 2
        total = total + (1 << bit) * (1 - digit if mask >> bit & 1 else digit)
    return total


def attention_kernel(
    pitch,
    table_ref,
    first_ref,
    second_ref,
    latent_ref,
    rotary_ref,
    latent_gain_ref,
    key_first_ref,
    value_first_ref,
    key_second_ref,
    value_second_ref,
    out_first_ref,
    out_second_ref,
    residual_ref,
    expert_gain_ref,
    route_ref,
    score_ref,
    middle_ref,
    normed_ref,
    codes_ref,
    latents,
    rotaries,
    queries,
    weights,
    residual,
    state,
    numerator,
    part,
    core_land,
    side_land,
    line_land,
    total,
    load_sem,
    cross_sem,
    cross_back,
    core_sem,
    side_sem,
    line_sem,
    send_sem,
):
    sets = lax.axis_size("tp")
    lines = sets // 4
    bits = lines.bit_length() - 1
    chunks, _, _, rows, width = part.shape
    _, seq_rows, rank = latents.shape
    first_nope, second_nope = key_first_ref.shape[0], key_second_ref.shape[1]
    first_width, second_width = value_first_ref.shape[0], value_second_ref.shape[1]
    half_turn = table_ref.shape[0] // 2
    rotary = 2 * half_turn
    sp, tp = lax.axis_index("sp"), lax.axis_index("tp")
    core, row, line = tp % 2, (tp // 2) % 2, tp // 4
    wide, narrow = jnp.float32, jnp.bfloat16

    at_line = [flipped(line, m, bits) for m in range(lines)]
    x_device = {"sp": 1 - sp, "tp": tp}
    y_device = {"sp": sp, "tp": line * 4 + (1 - row) * 2 + core}
    core_device = {"sp": sp, "tp": line * 4 + row * 2 + 1 - core}
    line_device = [{"sp": sp, "tp": at_line[m] * 4 + row * 2 + core} for m in range(lines)]

    barrier = pltpu.get_barrier_semaphore()
    everyone = [x_device, y_device, core_device] + line_device[1:]
    for one in everyone:
        pl.semaphore_signal(barrier, inc=1, device_id=one, device_id_type=MESH)

    own_rows = pl.ds(pl.multiple_of(tp * rows, rows), rows)
    loads = [
        pltpu.make_async_copy(source, target, load_sem.at[number])
        for number, (source, target) in enumerate(
            (
                (latent_ref, latents.at[0]),
                (out_first_ref, weights.at[:first_width, :]),
                (out_second_ref, weights.at[first_width:, :]),
                (residual_ref.at[own_rows, :], residual),
            )
        )
    ]
    for copy in loads:
        copy.start()

    def push(source, target, send, receive, where):
        copy = pltpu.make_async_remote_copy(
            src_ref=source,
            dst_ref=target,
            send_sem=send,
            recv_sem=receive,
            device_id=where,
            device_id_type=MESH,
        )
        copy.start()
        return copy

    def settle(view, sem):
        pltpu.make_async_copy(view, view, sem).wait()

    mine = pl.ds(pl.multiple_of(core * (seq_rows // 2), seq_rows // 2), seq_rows // 2)
    loads[0].wait()
    pl.semaphore_wait(barrier, len(everyone))

    @pl.when(sp == 0)
    def _():
        push(
            latents.at[0, mine, :],
            latents.at[1, mine, :],
            cross_back.at[0],
            cross_sem.at[0],
            x_device,
        )
        push(rotary_ref, rotaries, cross_back.at[1], cross_sem.at[1], x_device)

    tile = 4 * rows
    own_codes = codes_ref.at[sp]
    scores = score_ref[...]
    raised = jnp.exp(scores - jnp.max(scores, axis=0, keepdims=True))
    shares = raised / jnp.sum(raised, axis=0, keepdims=True)
    chosen = route_ref[...].astype(wide)
    upright = jnp.concatenate([chosen] * 4, axis=0).T
    earlier = lax.broadcasted_iota(jnp.int32, (tile, tile), 0)
    later = lax.broadcasted_iota(jnp.int32, (tile, tile), 1)
    counted = (earlier < later) & (earlier // rows == later // rows)
    places = lax.broadcasted_iota(jnp.int32, (1, seq_rows), 1)
    span_blocks = TILE_TOKENS // rows
    spots = (places // rows % span_blocks * CAP).astype(wide)
    lists = []
    for choice in range(2):
        ranks = []
        for start in range(0, seq_rows, tile):
            wanted = chosen[choice : choice + 1, start : start + tile]
            same = (upright[start : start + tile, 0:1] == wanted) | (
                upright[start : start + tile, 1:2] == wanted
            )
            ranks.append(jnp.sum(jnp.where(same & counted, 1.0, 0.0), axis=0, keepdims=True))
        lists.append(
            chosen[choice : choice + 1] * pitch + spots + jnp.concatenate(ranks, axis=1)
        )
    lists = jnp.concatenate(lists + [shares], axis=0)
    own_codes[...] = jnp.concatenate([lists, lists], axis=0)
    route_copy = push(own_codes, own_codes, cross_back.at[2], cross_sem.at[2], x_device)

    own_places = pl.ds(pl.multiple_of(sp * seq_rows, seq_rows), seq_rows)

    def turned(values, where):
        cosine, sine = table_ref[:half_turn, where], table_ref[half_turn:, where]
        upper, lower = values[:half_turn].astype(wide), values[half_turn:].astype(wide)
        return jnp.concatenate(
            [upper * cosine - lower * sine, lower * cosine + upper * sine], axis=0
        )

    first_end = first_nope + rotary
    queries[:first_nope] = first_ref[:first_nope]
    queries[first_nope:first_end] = turned(first_ref[first_nope:], own_places).astype(narrow)
    queries[first_end : first_end + second_nope] = second_ref[:second_nope]
    queries[first_end + second_nope :] = turned(second_ref[second_nope:], own_places).astype(narrow)
    value_second = value_second_ref[...].astype(wide).T.astype(narrow)
    across = (((1,), (1,)), ((), ()))

    def fold(slot, rotary_values, where, causal, fresh):
        raw = latents[slot].astype(wide)
        root = lax.rsqrt(jnp.mean(raw * raw, axis=-1, keepdims=True) + norm_epsilon)
        base = (raw * root * latent_gain_ref[...]).astype(narrow)
        turned_keys = turned(rotary_values, where).T.astype(narrow)
        if causal:
            key_places = lax.broadcasted_iota(jnp.int32, (seq_rows, seq_rows), 0)
            query_places = lax.broadcasted_iota(jnp.int32, (seq_rows, seq_rows), 1)
            allowed = key_places <= query_places
        for group in range(2):
            if group == 0:
                keys = lax.dot_general(base, key_first_ref[...], across, preferred_element_type=wide)
                values = lax.dot_general(
                    value_first_ref[...], base, across, preferred_element_type=wide
                )
                found = queries[:first_end]
                spots = pl.ds(0, first_width)
            else:
                keys = jnp.dot(base, key_second_ref[...], preferred_element_type=wide)
                values = lax.dot_general(value_second, base, across, preferred_element_type=wide)
                found = queries[first_end:]
                spots = pl.ds(first_width, second_width)
            keys = jnp.concatenate([keys.astype(narrow), turned_keys], axis=1)
            score = jnp.dot(keys, found, preferred_element_type=wide) * (
                keys.shape[1] ** (-0.5)
            )
            if causal:
                score = jnp.where(allowed, score, masked_score)
            highest = jnp.max(score, axis=0, keepdims=True)
            if not fresh:
                before = state[group : group + 1]
                highest = jnp.maximum(highest, before)
                kept = jnp.exp(before - highest)
            raised = jnp.exp(score - highest)
            amount = jnp.sum(raised, axis=0, keepdims=True)
            mixed = jnp.dot(
                values.astype(narrow), raised.astype(narrow), preferred_element_type=wide
            )
            if not fresh:
                amount = amount + kept * state[group + 2 : group + 3]
                mixed = mixed + kept * numerator[spots, :]
            state[group : group + 1] = highest
            state[group + 2 : group + 3] = amount
            numerator[spots, :] = mixed

    fold(0, rotary_ref[...], own_places, True, True)

    @pl.when(sp == 1)
    def _():
        there = latents.at[1, mine, :]
        settle(there, cross_sem.at[0])
        passed = push(there, there, cross_back.at[0], cross_sem.at[3], core_device)
        settle(rotaries, cross_sem.at[1])
        passed.wait_recv()
        fold(1, rotaries[...], pl.ds(0, seq_rows), False, False)
        passed.wait_send()

    @pl.when(sp == 0)
    def _():
        settle(latents.at[0, mine, :], cross_back.at[0])
        settle(rotary_ref, cross_back.at[1])

    attended = jnp.concatenate(
        [
            numerator[:first_width] / state[2:3],
            numerator[first_width:] / state[3:4],
        ],
        axis=0,
    )
    attended = attended.T.astype(narrow)
    loads[1].wait()
    loads[2].wait()

    def spot(chunk, at, up):
        return part.at[chunk, at * 2 + up, core]

    def add(chunk, at, up, extra):
        here = (chunk, at * 2 + up, core)
        part[here] = (part[here].astype(wide) + extra.astype(wide)).astype(narrow)

    def project(chunk):
        columns = slice(chunk * width, (chunk + 1) * width)
        found = jnp.dot(attended, weights[:, columns], preferred_element_type=wide)
        part[chunk] = found.astype(narrow).reshape(2 * lines, 2, rows, width)
        push(
            part.at[chunk, :, 1 - core],
            core_land.at[chunk],
            send_sem.at[chunk, 0],
            core_sem.at[chunk],
            core_device,
        )

    def to_side(chunk):
        settle(core_land.at[chunk], core_sem.at[chunk])
        for m in range(lines):
            add(chunk, at_line[m], 1 - row, core_land[chunk, at_line[m] * 2 + 1 - row])
            push(
                spot(chunk, at_line[m], 1 - row),
                side_land.at[chunk, m],
                send_sem.at[chunk, 1],
                side_sem.at[chunk, m],
                y_device,
            )
        for m in range(lines):
            add(chunk, at_line[m], row, core_land[chunk, at_line[m] * 2 + row])

    def to_line(chunk):
        for m in [*range(1, lines), 0]:
            settle(side_land.at[chunk, m], side_sem.at[chunk, m])
            value = part[chunk, at_line[m] * 2 + row, core].astype(wide) + side_land[
                chunk, m
            ].astype(wide)
            if m == 0:
                total[chunk] = value
                continue
            part[chunk, at_line[m] * 2 + row, core] = value.astype(narrow)
            push(
                spot(chunk, at_line[m], row),
                line_land.at[chunk, m - 1],
                send_sem.at[chunk, 2],
                line_sem.at[chunk, m - 1],
                line_device[m],
            )

    def close(chunk):
        value = total[chunk]
        for m in range(1, lines):
            settle(line_land.at[chunk, m - 1], line_sem.at[chunk, m - 1])
            value = value + line_land[chunk, m - 1].astype(wide)
        columns = slice(chunk * width, (chunk + 1) * width)
        middle_ref[:, columns] = (residual[:, columns].astype(wide) + value).astype(narrow)

    stages = (to_side, to_line, close)
    loads[3].wait()
    for step in range(chunks + len(stages)):
        if step < chunks:
            project(step)
        for number, stage in enumerate(stages):
            chunk = step - 1 - number
            if 0 <= chunk < chunks:
                stage(chunk)
    middle = middle_ref[...].astype(wide)
    root = lax.rsqrt(jnp.mean(middle * middle, axis=-1, keepdims=True) + norm_epsilon)
    normed_ref[...] = (middle * root * expert_gain_ref[...]).astype(narrow)
    for chunk in range(chunks):
        settle(core_land.at[chunk], send_sem.at[chunk, 0])
        settle(side_land.at[chunk], send_sem.at[chunk, 1])
        settle(line_land.at[chunk], send_sem.at[chunk, 2])
    route_copy.wait_send()
    settle(codes_ref.at[0], cross_sem.at[2])


def run_attention(table, arguments, rows, pitch, chunks, collective_id):
    (first, second, latent, rotary, _, _, value_first, _, value_second) = arguments[:9]
    residual = arguments[11]
    groups, sets = lax.axis_size("sp"), lax.axis_size("tp")
    lines = sets // 4
    seq_rows, rank = latent.shape
    depth = residual.shape[1]
    width = depth // chunks
    heads = value_first.shape[0] + value_second.shape[1]
    narrow, wide = jnp.bfloat16, jnp.float32
    anywhere = pl.BlockSpec(memory_space=pl.ANY)
    dma = pltpu.SemaphoreType.DMA
    specs = [VMEM] * (1 + len(arguments))
    for place in (2, 9, 10, 11):
        specs[1 + place] = anywhere
    return pl.pallas_call(
        functools.partial(attention_kernel, pitch),
        out_shape=(
            jax.ShapeDtypeStruct((rows, depth), narrow),
            jax.ShapeDtypeStruct((rows, depth), narrow),
            jax.ShapeDtypeStruct((groups, 8, seq_rows), wide),
        ),
        in_specs=specs,
        out_specs=(VMEM,) * 3,
        scratch_shapes=[
            pltpu.VMEM((2, seq_rows, rank), narrow),
            pltpu.VMEM(rotary.shape, narrow),
            pltpu.VMEM((first.shape[0] + second.shape[0], seq_rows), narrow),
            pltpu.VMEM((heads, depth), narrow),
            pltpu.VMEM((rows, depth), narrow),
            pltpu.VMEM((8, seq_rows), wide),
            pltpu.VMEM((heads, seq_rows), wide),
            pltpu.VMEM((chunks, 2 * lines, 2, rows, width), narrow),
            pltpu.VMEM((chunks, 2 * lines, rows, width), narrow),
            pltpu.VMEM((chunks, lines, rows, width), narrow),
            pltpu.VMEM((chunks, lines - 1, rows, width), narrow),
            pltpu.VMEM((chunks, rows, width), wide),
            dma((4,)),
            dma((4,)),
            dma((3,)),
            dma((chunks,)),
            dma((chunks, lines)),
            dma((chunks, lines - 1)),
            dma((chunks, 3)),
        ],
        compiler_params=pltpu.CompilerParams(
            collective_id=collective_id, has_side_effects=True, vmem_limit_bytes=40 << 20
        ),
        name="run_attention",
    )(table, *arguments)


def mixture_kernel(
    pitch,
    x_ref,
    middle_ref,
    code_ref,
    gate_ref,
    up_ref,
    down_ref,
    out_ref,
    tok,
    hot,
    hot_turned,
    scale,
    picked,
    gate_sum,
    up_sum,
    active,
    gate_buf,
    up_buf,
    down_buf,
    core_land,
    diag_land,
    side_land,
    line_land,
    own_sum,
    line_sem,
    side_sem,
    diag_sem,
    core_sem,
    pass_sem,
    core_back,
    diag_back,
    side_back,
    line_back,
    send_back,
    weight_sem,
    down_sem,
):
    groups, sets = lax.axis_size("sp"), lax.axis_size("tp")
    lines = sets // 4
    bits = lines.bit_length() - 1
    chunks, pairs, _, rows, width = tok.shape
    experts = picked.shape[0]
    tiles, span, tokens = hot.shape
    per_tile = tokens // (2 * rows)
    half = lines // 2
    sp, tp = lax.axis_index("sp"), lax.axis_index("tp")
    core, row, line = tp % 2, (tp // 2) % 2, tp // 4

    def device(side, at, up, half_chip):
        return {"sp": side, "tp": at * 4 + up * 2 + half_chip}

    def pair_of(side, at, up):
        return side * (sets // 2) + at * 2 + up

    at_line = [flipped(line, m, bits) for m in range(lines)]
    own = [pair_of(sp, at_line[m], row) for m in range(lines)]
    by_x = [pair_of(1 - sp, at_line[m], row) for m in range(lines)]
    by_y = [pair_of(sp, at_line[m], 1 - row) for m in range(lines)]
    by_xy = [pair_of(1 - sp, at_line[m], 1 - row) for m in range(lines)]
    x_device = device(1 - sp, line, row, core)
    y_device = device(sp, line, 1 - row, core)
    core_device = device(sp, line, row, 1 - core)
    line_device = [device(sp, at_line[m], row, core) for m in range(lines)]

    barrier = pltpu.get_barrier_semaphore()
    everyone = [x_device, y_device, core_device] + line_device[1:]
    for one in everyone:
        pl.semaphore_signal(barrier, inc=1, device_id=one, device_id_type=MESH)

    def weight_copies(chunk):
        part = pl.ds(chunk * width, width)
        slot = chunk % 2
        return (
            pltpu.make_async_copy(
                gate_ref.at[:, part, :], gate_buf.at[slot], weight_sem.at[slot, 0]
            ),
            pltpu.make_async_copy(up_ref.at[:, part, :], up_buf.at[slot], weight_sem.at[slot, 1]),
        )

    def down_copy(chunk):
        part = pl.ds(chunk * width, width)
        return pltpu.make_async_copy(
            down_ref.at[:, :, part], down_buf.at[chunk], down_sem.at[chunk]
        )

    for chunk in range(min(2, chunks)):
        for copy in weight_copies(chunk):
            copy.start()

    pl.semaphore_wait(barrier, len(everyone))

    def push(source, target, send, receive, where):
        pltpu.make_async_remote_copy(
            src_ref=source,
            dst_ref=target,
            send_sem=send,
            recv_sem=receive,
            device_id=where,
            device_id_type=MESH,
        ).start()

    def settle(view, sem):
        pltpu.make_async_copy(view, view, sem).wait()

    def spot(chunk, pair):
        return tok.at[chunk, pair, core]

    def share(chunk, pair, part):
        push(
            spot(chunk, pair),
            spot(chunk, pair),
            pass_sem.at[chunk, part],
            core_sem.at[chunk],
            core_device,
        )

    def send_own(chunk):
        source = x_ref.at[:, pl.ds(chunk * width, width)]
        target = spot(chunk, own[0])
        early = pass_sem.at[chunk, 0]
        for m in range(1, lines):
            push(source, target, early, line_sem.at[chunk, m - 1], line_device[m])
        push(source, target, early, side_sem.at[chunk, 0, 0], x_device)
        push(source, target, early, side_sem.at[chunk, 1, 0], y_device)
        push(source, target, early, core_sem.at[chunk], core_device)

    def pass_line(chunk):
        for m in range(1, lines):
            settle(spot(chunk, own[m]), line_sem.at[chunk, m - 1])
            here = spot(chunk, own[m])
            early = pass_sem.at[chunk, 0]
            push(here, here, early, side_sem.at[chunk, 0, m], x_device)
            push(here, here, early, side_sem.at[chunk, 1, m], y_device)
            share(chunk, own[m], 0)

    def pass_side(chunk):
        for m in [*range(half, lines), *range(half)]:
            turn = ((0, by_x), (1, by_y)) if m >= half else ((1, by_y), (0, by_x))
            for axis, column in turn:
                here = spot(chunk, column[m])
                settle(here, side_sem.at[chunk, axis, m])
                late = pass_sem.at[chunk, 1]
                if axis == 0 and m >= half:
                    push(here, here, late, diag_sem.at[chunk, m], y_device)
                if axis == 1 and m < half:
                    push(here, here, late, diag_sem.at[chunk, m], x_device)
                share(chunk, column[m], 1)

    def pass_diag(chunk):
        for m in range(lines):
            settle(spot(chunk, by_xy[m]), diag_sem.at[chunk, m])
            share(chunk, by_xy[m], 1)

    def finish(chunk):
        settle(tok.at[chunk, :, 0], core_sem.at[chunk])

    for chunk in range(chunks):
        send_own(chunk)
    for chunk in range(chunks):
        tok[chunk, own[0], core] = x_ref[:, chunk * width : (chunk + 1) * width]

    for tile in range(tiles):
        slots = lax.broadcasted_iota(jnp.int32, (span, tokens), 0)
        side, place = divmod(tile * tokens, code_ref.shape[2])
        code = code_ref[side, :, place : place + tokens]
        slots = slots + sp * span
        first = slots == code[0:1].astype(jnp.int32)
        second = slots == code[1:2].astype(jnp.int32)
        chosen = jnp.where(first | second, 1.0, 0.0)
        hot[tile] = chosen.astype(jnp.bfloat16)
        hot_turned[tile] = chosen.T.astype(jnp.bfloat16)
        portion = jnp.where(first, code[2:3], 0.0) + jnp.where(second, code[3:4], 0.0)
        scale[:, tile * pitch : (tile + 1) * pitch, :] = jnp.sum(
            portion, axis=1, keepdims=True
        ).reshape(experts, pitch, 1)

    def pick(chunk, tile):
        block = tok[chunk, tile * per_tile : (tile + 1) * per_tile].reshape(tokens, width)
        found = jnp.dot(hot[tile], block, preferred_element_type=jnp.float32)
        picked[:, tile * pitch : (tile + 1) * pitch, :] = found.astype(jnp.bfloat16).reshape(
            experts, pitch, width
        )

    def hidden(chunk, low, high):
        slot = chunk % 2

        def one(expert, carry):
            block = picked[expert]
            gate = jnp.dot(block, gate_buf[slot, expert], preferred_element_type=jnp.float32)
            upward = jnp.dot(block, up_buf[slot, expert], preferred_element_type=jnp.float32)
            if chunk > 0:
                gate = gate + gate_sum[expert]
                upward = upward + up_sum[expert]
            if chunk + 1 < chunks:
                gate_sum[expert] = gate
                up_sum[expert] = upward
            else:
                active[expert] = clamped_unit(gate, upward).astype(jnp.bfloat16)
            return carry

        lax.fori_loop(low, high, one, 0, unroll=2)

    pass_line(0)
    if chunks > 1:
        pass_line(1)
    pass_side(0)
    if chunks > 2:
        pass_line(2)
    pass_diag(0)
    for chunk in range(chunks):
        finish(chunk)
        for tile in range(tiles):
            pick(chunk, tile)
        if chunk + 1 < chunks:
            pass_side(chunk + 1)
        for copy in weight_copies(chunk):
            copy.wait()
        hidden(chunk, 0, experts // 2)
        if chunk + 3 < chunks:
            pass_line(chunk + 3)
        if chunk + 1 < chunks:
            pass_diag(chunk + 1)
        hidden(chunk, experts // 2, experts)
        if chunk + 2 < chunks:
            for copy in weight_copies(chunk + 2):
                copy.start()
        if chunk == 0:
            for later in range(chunks):
                down_copy(later).start()

    for chunk in range(chunks):
        settle(tok.at[chunk, : pairs - 1, 0], pass_sem.at[chunk, 0])
        settle(tok.at[chunk, :, 0], pass_sem.at[chunk, 1])

    def lower(chunk):
        down_copy(chunk).wait()

        def one(expert, carry):
            result = jnp.dot(
                active[expert], down_buf[chunk, expert], preferred_element_type=jnp.float32
            )
            picked[expert] = (result * scale[expert]).astype(jnp.bfloat16)
            return carry

        lax.fori_loop(0, experts, one, 0, unroll=2)
        for tile in range(tiles):
            block = picked[:, tile * pitch : (tile + 1) * pitch, :].reshape(span, width)
            total = jnp.dot(hot_turned[tile], block, preferred_element_type=jnp.float32)
            tok[chunk, tile * per_tile : (tile + 1) * per_tile] = total.astype(
                jnp.bfloat16
            ).reshape(per_tile, 2, rows, width)

    def meet_core(chunk):
        push(
            tok.at[chunk, :, 1 - core],
            core_land.at[chunk],
            send_back.at[chunk, 0],
            core_back.at[chunk],
            core_device,
        )

    def add_core(chunk, pair):
        tok[chunk, pair, core] = (
            tok[chunk, pair, core].astype(jnp.float32) + core_land[chunk, pair].astype(jnp.float32)
        ).astype(jnp.bfloat16)

    def back_diag(chunk):
        settle(core_land.at[chunk], core_back.at[chunk])
        send = send_back.at[chunk, 1]
        for m in range(lines):
            add_core(chunk, by_xy[m])
            push(
                spot(chunk, by_xy[m]),
                diag_land.at[chunk, m],
                send,
                diag_back.at[chunk, m],
                y_device if m >= half else x_device,
            )
        for m in range(lines):
            axis, column, where = (1, by_y, y_device) if m >= half else (0, by_x, x_device)
            add_core(chunk, column[m])
            push(
                spot(chunk, column[m]),
                side_land.at[chunk, axis, m],
                send,
                side_back.at[chunk, axis, m],
                where,
            )
        for m in range(lines):
            add_core(chunk, (by_x if m >= half else by_y)[m])
            add_core(chunk, own[m])

    def back_side(chunk):
        for m in range(lines):
            axis, column, where = (0, by_x, x_device) if m >= half else (1, by_y, y_device)
            settle(diag_land.at[chunk, m], diag_back.at[chunk, m])
            tok[chunk, column[m], core] = (
                tok[chunk, column[m], core].astype(jnp.float32)
                + diag_land[chunk, m].astype(jnp.float32)
            ).astype(jnp.bfloat16)
            push(
                spot(chunk, column[m]),
                side_land.at[chunk, axis, m],
                send_back.at[chunk, 2],
                side_back.at[chunk, axis, m],
                where,
            )

    def back_line(chunk):
        for m in [*range(1, lines), 0]:
            total = tok[chunk, own[m], core].astype(jnp.float32)
            for axis in range(2):
                settle(side_land.at[chunk, axis, m], side_back.at[chunk, axis, m])
                total = total + side_land[chunk, axis, m].astype(jnp.float32)
            if m == 0:
                own_sum[chunk] = total
                continue
            tok[chunk, own[m], core] = total.astype(jnp.bfloat16)
            push(
                spot(chunk, own[m]),
                line_land.at[chunk, m - 1],
                send_back.at[chunk, 3],
                line_back.at[chunk, m - 1],
                line_device[m],
            )

    def close(chunk):
        total = own_sum[chunk]
        for m in range(1, lines):
            settle(line_land.at[chunk, m - 1], line_back.at[chunk, m - 1])
            total = total + line_land[chunk, m - 1].astype(jnp.float32)
        part = slice(chunk * width, (chunk + 1) * width)
        out_ref[:, part] = (middle_ref[:, part].astype(jnp.float32) + total).astype(jnp.bfloat16)

    stages = (back_diag, back_side, back_line, close)
    for step in range(chunks + len(stages)):
        if step < chunks:
            lower(step)
            meet_core(step)
        for number, stage in enumerate(stages):
            chunk = step - 1 - number
            if 0 <= chunk < chunks:
                stage(chunk)
    for chunk in range(chunks):
        settle(core_land.at[chunk], send_back.at[chunk, 0])
        settle(tok.at[chunk, : 2 * lines, 0], send_back.at[chunk, 1])
        settle(tok.at[chunk, :lines, 0], send_back.at[chunk, 2])
        settle(tok.at[chunk, : lines - 1, 0], send_back.at[chunk, 3])


def run_mixture(
    tokens, middle, codes, gate_weight, up_weight, down_weight, pitch, chunks, collective_id
):
    experts, depth, units = gate_weight.shape
    rows = tokens.shape[0]
    groups, sets = lax.axis_size("sp"), lax.axis_size("tp")
    tile_tokens = TILE_TOKENS
    tiles = groups * sets * rows // tile_tokens
    pairs, lines = groups * sets // 2, sets // 4
    width = depth // chunks
    span = experts * pitch
    narrow, wide = jnp.bfloat16, jnp.float32
    anywhere = pl.BlockSpec(memory_space=pl.ANY)
    dma = pltpu.SemaphoreType.DMA
    return pl.pallas_call(
        functools.partial(mixture_kernel, pitch),
        out_shape=jax.ShapeDtypeStruct(tokens.shape, jnp.bfloat16),
        in_specs=[VMEM, VMEM, VMEM, anywhere, anywhere, anywhere],
        out_specs=VMEM,
        scratch_shapes=[
            pltpu.VMEM((chunks, pairs, 2, rows, width), narrow),
            pltpu.VMEM((tiles, span, tile_tokens), narrow),
            pltpu.VMEM((tiles, tile_tokens, span), narrow),
            pltpu.VMEM((experts, tiles * pitch, 1), wide),
            pltpu.VMEM((experts, tiles * pitch, width), narrow),
            pltpu.VMEM((experts, tiles * pitch, units), wide),
            pltpu.VMEM((experts, tiles * pitch, units), wide),
            pltpu.VMEM((experts, tiles * pitch, units), narrow),
            pltpu.VMEM((2, experts, width, units), narrow),
            pltpu.VMEM((2, experts, width, units), narrow),
            pltpu.VMEM((chunks, experts, units, width), narrow),
            pltpu.VMEM((chunks, pairs, rows, width), narrow),
            pltpu.VMEM((chunks, lines, rows, width), narrow),
            pltpu.VMEM((chunks, 2, lines, rows, width), narrow),
            pltpu.VMEM((chunks, lines - 1, rows, width), narrow),
            pltpu.VMEM((chunks, rows, width), wide),
            dma((chunks, lines - 1)),
            dma((chunks, 2, lines)),
            dma((chunks, lines)),
            dma((chunks,)),
            dma((chunks, 2)),
            dma((chunks,)),
            dma((chunks, lines)),
            dma((chunks, 2, lines)),
            dma((chunks, lines - 1)),
            dma((chunks, 4)),
            dma((2, 2)),
            dma((chunks,)),
        ],
        compiler_params=pltpu.CompilerParams(
            collective_id=collective_id, has_side_effects=True, vmem_limit_bytes=63 << 20
        ),
        name="run_mixture",
    )(tokens, middle, codes, gate_weight, up_weight, down_weight)


def token_body(
    query_first,
    query_second,
    latent,
    key_rotary,
    latent_gain,
    key_up_first,
    value_up_first,
    key_up_second,
    value_up_second,
    out_first,
    out_second,
    residual,
    expert_gain,
    route_experts,
    route_scores,
    gate_weight,
    up_weight,
    down_weight,
):
    seq_rows = latent.shape[0]
    sets = lax.axis_size("tp")
    groups = lax.axis_size("sp")
    own_rows = seq_rows // sets
    span_blocks = TILE_TOKENS // own_rows
    pitch = -(-span_blocks * CAP // 16) * 16
    half = key_rotary.shape[1] // 2
    inverse = np.float32(rotary_base) ** (-np.arange(half, dtype=np.float32) / half)
    angles = inverse[:, None] * np.arange(groups * seq_rows, dtype=np.float32)[None, :]
    table = np.concatenate([np.cos(angles), np.sin(angles)], axis=0).astype(np.float32)
    middle, normed, codes = run_attention(
        jnp.asarray(table),
        (
            query_first.T,
            query_second.T,
            latent,
            key_rotary.T,
            latent_gain[None, :],
            key_up_first.T,
            value_up_first.T,
            key_up_second,
            value_up_second,
            out_first,
            out_second,
            residual,
            expert_gain[None, :],
            route_experts.T,
            route_scores.T,
        ),
        own_rows,
        pitch,
        CHUNKS,
        1,
    )
    return run_mixture(
        normed, middle, codes, gate_weight, up_weight, down_weight, pitch, CHUNKS, 2
    )


def solution(mesh):
    in_specs = (
        P("sp", "tp"),
        P("sp", "tp"),
        P("sp", None),
        P("sp", None),
        P(),
        P(None, "tp"),
        P(None, "tp"),
        P(None, "tp"),
        P(None, "tp"),
        P("tp", None),
        P("tp", None),
        P("sp", None),
        P(),
        P("sp", None),
        P("sp", None),
        P("sp", None, "tp"),
        P("sp", None, "tp"),
        P("sp", "tp", None),
    )
    out_specs = P(("sp", "tp"), None)
    groups, sets = mesh.shape["sp"], mesh.shape["tp"]
    small = groups == 2 and sets & (sets - 1) == 0 and sets > 4

    def body(*arguments):
        fits = small and arguments[2].shape[0] * groups <= 1024
        return (token_body if fits else slot_body)(*arguments)

    return jax.shard_map(body, mesh=mesh, in_specs=in_specs, out_specs=out_specs, check_vma=False)
```

```python
import functools

import jax
import jax.numpy as jnp
import numpy as np
from jax import lax
from jax.experimental import pallas as pl
from jax.experimental.pallas import tpu as pltpu
from jax.sharding import PartitionSpec as P

NA = 64
NB = 128
ROPE = 32
CAP = 3


norm_epsilon = 1e-06
rotary_base = 10000.0
clamp_limit = 7.0
sigmoid_slope = 1.702
masked_score = -1e30


def rotate(values, positions):
    half = values.shape[-1] // 2
    inverse = rotary_base ** (-jnp.arange(half, dtype=jnp.float32) / half)
    angles = positions.astype(jnp.float32)[:, None, None] * inverse[None, None, :]
    cosine = jnp.cos(angles)
    sine = jnp.sin(angles)
    first = values[..., :half]
    second = values[..., half:]
    return jnp.concatenate(
        [first * cosine - second * sine, second * cosine + first * sine], axis=-1
    )


def rms_scaled(values, gain):
    wide = values.astype(jnp.float32)
    return wide * lax.rsqrt(jnp.mean(wide * wide, axis=-1, keepdims=True) + norm_epsilon) * gain


def turned_queries(query, nope, positions):
    shaped = query.reshape(query.shape[0], query.shape[1] // (nope + ROPE), nope + ROPE)
    turned = rotate(shaped[..., nope:].astype(jnp.float32), positions).astype(jnp.bfloat16)
    return jnp.concatenate([shaped[..., :nope], turned], axis=-1)


def clamped_unit(gate, upward):
    limited = jnp.minimum(gate, clamp_limit)
    bounded = jnp.clip(upward, -clamp_limit, clamp_limit)
    return (bounded + 1.0) * limited * jax.nn.sigmoid(sigmoid_slope * limited)


def slot_numbers(chosen, experts):
    hits = (chosen[..., None] == jnp.arange(experts, dtype=jnp.int32)).astype(jnp.int32)
    before = jnp.cumsum(hits, axis=-2) - hits
    return chosen * CAP + jnp.sum(before * hits, axis=-1)


def fold_group(state, queries, key_nope, key_turned, values, query_places, scale):
    running, denominator, numerator = state
    heads = queries.shape[1]
    nope = queries.shape[2] - key_turned.shape[1]
    keys = key_nope.reshape(key_nope.shape[0], heads, nope)
    value_rows = values.reshape(values.shape[0], heads, values.shape[1] // heads)
    score = jnp.einsum(
        "qhd,khd->qhk", queries[..., :nope], keys, preferred_element_type=jnp.float32
    )
    score = score + jnp.einsum(
        "qhr,kr->qhk", queries[..., nope:], key_turned, preferred_element_type=jnp.float32
    )
    score = score * scale
    key_places = jnp.arange(keys.shape[0], dtype=jnp.int32)
    allowed = (query_places[:, None] >= key_places[None, :])[:, None, :]
    score = jnp.where(allowed, score, masked_score)
    highest = jnp.maximum(running, jnp.max(score, axis=-1))
    weights = jnp.where(allowed, jnp.exp(score - highest[..., None]), 0.0)
    denominator = jnp.sum(weights, axis=-1)
    numerator = jnp.einsum(
        "qhk,khd->qhd", weights.astype(jnp.bfloat16), value_rows, preferred_element_type=jnp.float32
    )
    return (highest, denominator, numerator)


def expert_hidden(rows, gate_weight, up_weight):
    gate = jnp.einsum("nsecd,edf->nsecf", rows, gate_weight, preferred_element_type=jnp.float32)
    upward = jnp.einsum("nsecd,edf->nsecf", rows, up_weight, preferred_element_type=jnp.float32)
    return clamped_unit(gate, upward).astype(jnp.bfloat16)


def slot_body(
    query_first,
    query_second,
    latent,
    key_rotary,
    latent_gain,
    key_up_first,
    value_up_first,
    key_up_second,
    value_up_second,
    out_first,
    out_second,
    residual,
    expert_gain,
    route_experts,
    route_scores,
    gate_weight,
    up_weight,
    down_weight,
):
    seq_rows = latent.shape[0]
    sets = lax.axis_size("tp")
    groups = lax.axis_size("sp")
    own_rows = seq_rows // sets
    topk = route_experts.shape[1]
    local_experts = gate_weight.shape[0]
    experts = local_experts * groups
    offset = lax.axis_index("sp") * seq_rows
    places = offset + jnp.arange(seq_rows, dtype=jnp.int32)
    last_place = offset + seq_rows - 1
    queries_first = turned_queries(query_first, NA, places)
    queries_second = turned_queries(query_second, NB, places)
    key_turned = rotate(key_rotary.astype(jnp.float32)[:, None, :], places)[:, 0, :].astype(
        jnp.bfloat16
    )
    latent_normed = rms_scaled(latent, latent_gain).astype(jnp.bfloat16)
    scale_first = (NA + ROPE) ** (-0.5)
    scale_second = (NB + ROPE) ** (-0.5)

    def attend(carry, parts):
        key_first, value_first, key_second, value_second, turned = parts
        return (
            fold_group(
                carry[0], queries_first, key_first, turned, value_first, places, scale_first
            ),
            fold_group(
                carry[1], queries_second, key_second, turned, value_second, places, scale_second
            ),
        )

    def initial(queries, value_width):
        shape = queries.shape[:2]
        return (
            jnp.full(shape, masked_score, jnp.float32),
            jnp.zeros(shape, jnp.float32),
            jnp.zeros(shape + (value_width,), jnp.float32),
        )

    start_state = (
        initial(queries_first, value_up_first.shape[1] // queries_first.shape[1]),
        initial(queries_second, value_up_second.shape[1] // queries_second.shape[1]),
    )
    key_first, value_first, key_second, value_second = tuple(
        (
            jnp.dot(latent_normed, weight, preferred_element_type=jnp.float32).astype(jnp.bfloat16)
            for weight in (key_up_first, value_up_first, key_up_second, value_up_second)
        )
    )
    parts = (
        lax.all_gather(key_first, "sp", axis=0, tiled=True),
        lax.all_gather(value_first, "sp", axis=0, tiled=True),
        lax.all_gather(key_second, "sp", axis=0, tiled=True),
        lax.all_gather(value_second, "sp", axis=0, tiled=True),
        lax.all_gather(key_turned, "sp", axis=0, tiled=True),
    )
    state = lax.cond(
        jnp.int32(0) <= last_place,
        lambda inner: attend(inner, parts),
        lambda inner: inner,
        start_state,
    )
    first_state, second_state = state
    attended_first = (
        (first_state[2] / first_state[1][..., None]).astype(jnp.bfloat16).reshape(seq_rows, -1)
    )
    attended_second = (
        (second_state[2] / second_state[1][..., None]).astype(jnp.bfloat16).reshape(seq_rows, -1)
    )
    own_start = lax.axis_index("tp") * own_rows
    slot_range = jnp.arange(experts * CAP, dtype=jnp.int32)
    projected = lax.psum_scatter(
        (
            jnp.dot(attended_first, out_first, preferred_element_type=jnp.float32)
            + jnp.dot(attended_second, out_second, preferred_element_type=jnp.float32)
        ).astype(jnp.bfloat16),
        "tp",
        scatter_dimension=0,
        tiled=True,
    ).astype(jnp.float32)
    own_residual = lax.dynamic_slice_in_dim(residual, own_start, own_rows, 0)
    middle = (own_residual.astype(jnp.float32) + projected).astype(jnp.bfloat16)
    normed = rms_scaled(middle, expert_gain).astype(jnp.bfloat16)
    own_ids = lax.dynamic_slice_in_dim(route_experts, own_start, own_rows, 0).reshape(-1)
    own_slots = slot_numbers(own_ids, experts)
    picks = (own_slots[:, None] == slot_range).reshape(own_rows, topk, experts * CAP)
    selected = jnp.sum(picks.astype(jnp.float32), axis=1).astype(jnp.bfloat16)
    outgoing = jnp.einsum("ts,td->sd", selected, normed, preferred_element_type=jnp.float32).astype(
        jnp.bfloat16
    )
    outgoing = outgoing.reshape(groups, local_experts, CAP, outgoing.shape[-1])
    arrived = lax.all_to_all(outgoing, "sp", split_axis=0, concat_axis=0, tiled=True)
    activated = expert_hidden(
        lax.all_gather(arrived[None], "tp", axis=0, tiled=True), gate_weight, up_weight
    )
    flat_hidden = activated.reshape(sets * groups, local_experts, CAP, activated.shape[-1])
    summed = lax.psum_scatter(
        jnp.einsum(
            "secf,efd->secd", flat_hidden, down_weight, preferred_element_type=jnp.float32
        ).astype(jnp.bfloat16),
        "tp",
        scatter_dimension=0,
        tiled=True,
    )
    returned = lax.all_to_all(summed, "sp", split_axis=0, concat_axis=0, tiled=True)
    expert_out = returned.reshape(experts * CAP, returned.shape[-1]).astype(jnp.float32)
    own_scores = lax.dynamic_slice_in_dim(route_scores, own_start, own_rows, 0)
    route_weight = jax.nn.softmax(own_scores, axis=-1)
    matches = own_slots.reshape(own_rows, topk)[..., None] == slot_range
    combine = jnp.sum(jnp.where(matches, route_weight[..., None], 0.0), axis=1)
    mixture = jnp.dot(combine, expert_out, precision=lax.Precision.HIGHEST)
    return (middle.astype(jnp.float32) + mixture).astype(jnp.bfloat16)


MESH = pl.DeviceIdType.MESH
VMEM = pl.BlockSpec(memory_space=pltpu.VMEM)
TILE_TOKENS = 256
CHUNKS = 4
JOINT = 4
STRIPS = 4
LAGS = (1, 2, 0)


def flipped(value, mask, bits):
    total = 0
    for bit in range(bits):
        digit = (value // (1 << bit)) % 2
        total = total + (1 << bit) * (1 - digit if mask >> bit & 1 else digit)
    return total


def attention_kernel(
    pitch,
    table_ref,
    first_ref,
    second_ref,
    rotary_ref,
    latent_gain_ref,
    key_first_ref,
    value_first_ref,
    key_second_ref,
    value_second_ref,
    expert_gain_ref,
    route_ref,
    score_ref,
    loads,
    middle_ref,
    normed_ref,
    codes_ref,
    latents,
    rotaries,
    queries,
    weights,
    residual,
    state,
    numerator,
    part,
    core_land,
    side_land,
    line_land,
    total,
    cross_sem,
    cross_back,
    core_sem,
    side_sem,
    line_sem,
    send_sem,
):
    sets = lax.axis_size("tp")
    lines = sets // 4
    bits = lines.bit_length() - 1
    chunks, _, _, _, rows, width = part.shape
    _, seq_rows, rank = latents.shape
    first_nope, second_nope = key_first_ref.shape[0], key_second_ref.shape[1]
    first_width, second_width = value_first_ref.shape[0], value_second_ref.shape[1]
    half_turn = table_ref.shape[0] // 2
    rotary = 2 * half_turn
    sp, tp = lax.axis_index("sp"), lax.axis_index("tp")
    core, row, line = tp % 2, (tp // 2) % 2, tp // 4
    wide, narrow = jnp.float32, jnp.bfloat16

    at_line = [flipped(line, m, bits) for m in range(lines)]
    x_device = {"sp": 1 - sp, "tp": tp}
    y_device = {"sp": sp, "tp": line * 4 + (1 - row) * 2 + core}
    core_device = {"sp": sp, "tp": line * 4 + row * 2 + 1 - core}
    line_device = [{"sp": sp, "tp": at_line[m] * 4 + row * 2 + core} for m in range(lines)]

    barrier = pltpu.get_barrier_semaphore()
    everyone = [x_device, y_device, core_device] + line_device[1:]
    for one in everyone:
        pl.semaphore_signal(barrier, inc=1, device_id=one, device_id_type=MESH)

    def push(source, target, send, receive, where):
        copy = pltpu.make_async_remote_copy(
            src_ref=source,
            dst_ref=target,
            send_sem=send,
            recv_sem=receive,
            device_id=where,
            device_id_type=MESH,
        )
        copy.start()
        return copy

    def settle(view, sem):
        pltpu.make_async_copy(view, view, sem).wait()

    mine = pl.ds(pl.multiple_of(core * (seq_rows // 2), seq_rows // 2), seq_rows // 2)
    loads["latent"].wait()
    loads["rotary"].wait()
    pl.semaphore_wait(barrier, len(everyone))

    @pl.when(sp == 0)
    def _():
        push(
            latents.at[0, mine, :],
            latents.at[1, mine, :],
            cross_back.at[0],
            cross_sem.at[0],
            x_device,
        )
        push(rotary_ref, rotaries, cross_back.at[1], cross_sem.at[1], x_device)

    for name in ("routes", "scores"):
        loads[name].wait()

    tile = 4 * rows
    own_codes = codes_ref.at[sp]
    scores = score_ref[...]
    raised = jnp.exp(scores - jnp.max(scores, axis=0, keepdims=True))
    shares = raised / jnp.sum(raised, axis=0, keepdims=True)
    chosen = route_ref[...].astype(wide)
    upright = jnp.concatenate([chosen] * 4, axis=0).T
    earlier = lax.broadcasted_iota(jnp.int32, (tile, tile), 0)
    later = lax.broadcasted_iota(jnp.int32, (tile, tile), 1)
    counted = (earlier < later) & (earlier // rows == later // rows)
    places = lax.broadcasted_iota(jnp.int32, (1, seq_rows), 1)
    span_blocks = TILE_TOKENS // rows
    spots = (places // rows % span_blocks * CAP).astype(wide)
    lists = []
    for choice in range(2):
        ranks = []
        for start in range(0, seq_rows, tile):
            wanted = chosen[choice : choice + 1, start : start + tile]
            same = (upright[start : start + tile, 0:1] == wanted) | (
                upright[start : start + tile, 1:2] == wanted
            )
            ranks.append(jnp.sum(jnp.where(same & counted, 1.0, 0.0), axis=0, keepdims=True))
        lists.append(
            chosen[choice : choice + 1] * pitch + spots + jnp.concatenate(ranks, axis=1)
        )
    lists = jnp.concatenate(lists + [shares], axis=0)
    own_codes[...] = jnp.concatenate([lists, lists], axis=0)
    route_copy = push(own_codes, own_codes, cross_back.at[2], cross_sem.at[2], x_device)

    for name in (
        "table",
        "first",
        "second",
        "latent_gain",
        "key_first",
        "value_first",
        "key_second",
        "value_second",
    ):
        loads[name].wait()
    own_places = pl.ds(pl.multiple_of(sp * seq_rows, seq_rows), seq_rows)

    def turned(values, where):
        cosine, sine = table_ref[:half_turn, where], table_ref[half_turn:, where]
        upper, lower = values[:half_turn].astype(wide), values[half_turn:].astype(wide)
        return jnp.concatenate(
            [upper * cosine - lower * sine, lower * cosine + upper * sine], axis=0
        )

    first_end = first_nope + rotary
    queries[:first_nope] = first_ref[:first_nope]
    queries[first_nope:first_end] = turned(first_ref[first_nope:], own_places).astype(narrow)
    queries[first_end : first_end + second_nope] = second_ref[:second_nope]
    queries[first_end + second_nope :] = turned(second_ref[second_nope:], own_places).astype(narrow)
    value_second = value_second_ref[...].astype(wide).T.astype(narrow)
    across = (((1,), (1,)), ((), ()))

    def fold(slot, rotary_values, where, causal, fresh):
        raw = latents[slot].astype(wide)
        root = lax.rsqrt(jnp.mean(raw * raw, axis=-1, keepdims=True) + norm_epsilon)
        base = (raw * root * latent_gain_ref[...]).astype(narrow)
        turned_keys = turned(rotary_values, where).T.astype(narrow)
        if causal:
            key_places = lax.broadcasted_iota(jnp.int32, (seq_rows, seq_rows), 0)
            query_places = lax.broadcasted_iota(jnp.int32, (seq_rows, seq_rows), 1)
            allowed = key_places <= query_places
        for group in range(2):
            if group == 0:
                keys = lax.dot_general(base, key_first_ref[...], across, preferred_element_type=wide)
                values = lax.dot_general(
                    value_first_ref[...], base, across, preferred_element_type=wide
                )
                found = queries[:first_end]
                spots = pl.ds(0, first_width)
            else:
                keys = jnp.dot(base, key_second_ref[...], preferred_element_type=wide)
                values = lax.dot_general(value_second, base, across, preferred_element_type=wide)
                found = queries[first_end:]
                spots = pl.ds(first_width, second_width)
            keys = jnp.concatenate([keys.astype(narrow), turned_keys], axis=1)
            score = jnp.dot(keys, found, preferred_element_type=wide) * (
                keys.shape[1] ** (-0.5)
            )
            if causal:
                score = jnp.where(allowed, score, masked_score)
            highest = jnp.max(score, axis=0, keepdims=True)
            if not fresh:
                before = state[group : group + 1]
                highest = jnp.maximum(highest, before)
                kept = jnp.exp(before - highest)
            raised = jnp.exp(score - highest)
            amount = jnp.sum(raised, axis=0, keepdims=True)
            mixed = jnp.dot(
                values.astype(narrow), raised.astype(narrow), preferred_element_type=wide
            )
            if not fresh:
                amount = amount + kept * state[group + 2 : group + 3]
                mixed = mixed + kept * numerator[spots, :]
            state[group : group + 1] = highest
            state[group + 2 : group + 3] = amount
            numerator[spots, :] = mixed

    fold(0, rotary_ref[...], own_places, True, True)

    @pl.when(sp == 1)
    def _():
        there = latents.at[1, mine, :]
        settle(there, cross_sem.at[0])
        passed = push(there, there, cross_back.at[0], cross_sem.at[3], core_device)
        settle(rotaries, cross_sem.at[1])
        passed.wait_recv()
        fold(1, rotaries[...], pl.ds(0, seq_rows), False, False)
        passed.wait_send()

    @pl.when(sp == 0)
    def _():
        settle(latents.at[0, mine, :], cross_back.at[0])
        settle(rotary_ref, cross_back.at[1])

    attended = jnp.concatenate(
        [
            numerator[:first_width] / state[2:3],
            numerator[first_width:] / state[3:4],
        ],
        axis=0,
    )
    attended = attended.T.astype(narrow)
    for name in ("out_first", "out_second", "residual", "expert_gain"):
        loads[name].wait()

    def project(chunk):
        columns = slice(chunk * width, (chunk + 1) * width)
        found = jnp.dot(attended, weights[:, columns], preferred_element_type=wide)
        part[chunk] = found.astype(narrow).reshape(lines, 2, 2, rows, width)
        push(
            part.at[chunk, :, :, 1 - core],
            core_land.at[chunk],
            send_sem.at[chunk, 0],
            core_sem.at[chunk],
            core_device,
        )

    def add_core(chunk, up):
        part[chunk, :, up, core] = (
            part[chunk, :, up, core].astype(wide) + core_land[chunk, :, up].astype(wide)
        ).astype(narrow)

    def to_side(chunk):
        settle(core_land.at[chunk], core_sem.at[chunk])
        add_core(chunk, 1 - row)
        push(
            part.at[chunk, :, 1 - row, core],
            side_land.at[chunk],
            send_sem.at[chunk, 1],
            side_sem.at[chunk],
            y_device,
        )
        add_core(chunk, row)

    def to_line(chunk):
        settle(side_land.at[chunk], side_sem.at[chunk])
        total[chunk] = part[chunk, line, row, core].astype(wide) + side_land[chunk, line].astype(
            wide
        )
        part[chunk, :, row, core] = (
            part[chunk, :, row, core].astype(wide) + side_land[chunk].astype(wide)
        ).astype(narrow)
        for m in range(1, lines):
            push(
                part.at[chunk, at_line[m], row, core],
                line_land.at[chunk, m - 1],
                send_sem.at[chunk, 2],
                line_sem.at[chunk, m - 1],
                line_device[m],
            )

    def close(chunk):
        value = total[chunk]
        for m in range(1, lines):
            settle(line_land.at[chunk, m - 1], line_sem.at[chunk, m - 1])
            value = value + line_land[chunk, m - 1].astype(wide)
        columns = slice(chunk * width, (chunk + 1) * width)
        middle_ref[:, columns] = (residual[:, columns].astype(wide) + value).astype(narrow)

    stages = (to_side, to_line, close)
    for step in range(chunks + len(stages)):
        if step < chunks:
            project(step)
        for number, stage in enumerate(stages):
            chunk = step - 1 - number
            if 0 <= chunk < chunks:
                stage(chunk)
    middle = middle_ref[...].astype(wide)
    root = lax.rsqrt(jnp.mean(middle * middle, axis=-1, keepdims=True) + norm_epsilon)
    normed_ref[...] = (middle * root * expert_gain_ref[...]).astype(narrow)
    for chunk in range(chunks):
        settle(core_land.at[chunk], send_sem.at[chunk, 0])
        settle(side_land.at[chunk], send_sem.at[chunk, 1])
        settle(line_land.at[chunk], send_sem.at[chunk, 2])
    route_copy.wait_send()
    settle(codes_ref.at[0], cross_sem.at[2])


def mixture_kernel(
    pitch,
    weight_copies,
    x_ref,
    code_ref,
    down_ref,
    out_ref,
    tok,
    hot,
    hot_turned,
    scale,
    picked,
    gate_sum,
    up_sum,
    active,
    gate_buf,
    up_buf,
    down_buf,
    core_land,
    diag_land,
    side_land,
    line_land,
    own_sum,
    line_sem,
    side_sem,
    diag_sem,
    core_sem,
    pass_sem,
    core_back,
    diag_back,
    side_back,
    line_back,
    send_back,
    down_sem,
):
    groups, sets = lax.axis_size("sp"), lax.axis_size("tp")
    lines = sets // 4
    bits = lines.bit_length() - 1
    chunks, _, _, _, _, rows, width = tok.shape
    experts = picked.shape[0]
    tiles, span, tokens = hot.shape
    per_tile = tokens // (4 * rows)
    half = lines // 2
    sp, tp = lax.axis_index("sp"), lax.axis_index("tp")
    core, row, line = tp % 2, (tp // 2) % 2, tp // 4

    def device(side, at, up, half_chip):
        return {"sp": side, "tp": at * 4 + up * 2 + half_chip}

    at_line = [flipped(line, m, bits) for m in range(lines)]
    high = line // half
    near = pl.ds(high * half, half)
    far = pl.ds((1 - high) * half, half)
    whole = slice(None)
    x_device = device(1 - sp, line, row, core)
    y_device = device(sp, line, 1 - row, core)
    core_device = device(sp, line, row, 1 - core)
    line_device = [device(sp, at_line[m], row, core) for m in range(lines)]

    def down_copy(chunk):
        part = pl.ds(chunk * width, width)
        return pltpu.make_async_copy(
            down_ref.at[:, :, part], down_buf.at[chunk], down_sem.at[chunk]
        )

    def push(source, target, send, receive, where):
        pltpu.make_async_remote_copy(
            src_ref=source,
            dst_ref=target,
            send_sem=send,
            recv_sem=receive,
            device_id=where,
            device_id_type=MESH,
        ).start()

    def settle(view, sem):
        pltpu.make_async_copy(view, view, sem).wait()

    def share(chunk, side, up, number):
        column = tok.at[chunk, side, :, up, core]
        push(column, column, pass_sem.at[chunk, 3], core_sem.at[chunk, number], core_device)

    def send_own(chunk):
        source = x_ref.at[:, pl.ds(chunk * width, width)]
        target = tok.at[chunk, sp, line, row, core]
        for m in range(1, lines):
            push(source, target, pass_sem.at[chunk, 2], line_sem.at[chunk, m - 1], line_device[m])
        push(source, target, pass_sem.at[chunk, 0], side_sem.at[chunk, 0, 0], x_device)
        push(source, target, pass_sem.at[chunk, 0], side_sem.at[chunk, 1, 0], y_device)

    def pass_line(chunk):
        def onward(here, number):
            early = pass_sem.at[chunk, 0]
            push(here, here, early, side_sem.at[chunk, 0, number], x_device)
            push(here, here, early, side_sem.at[chunk, 1, number], y_device)

        for m in range(1, lines):
            here = tok.at[chunk, sp, at_line[m], row, core]
            settle(here, line_sem.at[chunk, m - 1])
            if m < half:
                onward(here, m)
        onward(tok.at[chunk, sp, far, row, core], half)
        share(chunk, sp, row, 0)

    def settle_near(chunk, axis, side, up):
        for m in range(half):
            settle(tok.at[chunk, side, at_line[m], up, core], side_sem.at[chunk, axis, m])

    def pass_side(chunk):
        by_x, by_y = (chunk, 1 - sp), (chunk, sp)
        late = pass_sem.at[chunk, 1]
        settle_near(chunk, 1, sp, 1 - row)
        here = tok.at[(*by_y, near, 1 - row, core)]
        push(here, here, late, diag_sem.at[chunk, 1], x_device)
        here = tok.at[(*by_x, far, row, core)]
        settle(here, side_sem.at[chunk, 0, half])
        push(here, here, late, diag_sem.at[chunk, 0], y_device)
        settle_near(chunk, 0, 1 - sp, row)
        share(chunk, 1 - sp, row, 1)
        settle(tok.at[(*by_y, far, 1 - row, core)], side_sem.at[chunk, 1, half])
        share(chunk, sp, 1 - row, 2)

    def pass_diag(chunk):
        for number, part in enumerate((far, near)):
            settle(tok.at[chunk, 1 - sp, part, 1 - row, core], diag_sem.at[chunk, number])
        share(chunk, 1 - sp, 1 - row, 3)

    def finish(chunk):
        for number in range(4):
            settle(tok.at[chunk, 0, :, 0, 0], core_sem.at[chunk, number])

    for chunk in range(chunks):
        send_own(chunk)
    for chunk in range(chunks):
        tok[chunk, sp, line, row, core] = x_ref[:, chunk * width : (chunk + 1) * width]

    for tile in range(tiles):
        slots = lax.broadcasted_iota(jnp.int32, (span, tokens), 0)
        side, place = divmod(tile * tokens, code_ref.shape[2])
        code = code_ref[side, :, place : place + tokens]
        slots = slots + sp * span
        first = slots == code[0:1].astype(jnp.int32)
        second = slots == code[1:2].astype(jnp.int32)
        chosen = jnp.where(first | second, 1.0, 0.0)
        hot[tile] = chosen.astype(jnp.bfloat16)
        hot_turned[tile] = chosen.T.astype(jnp.bfloat16)
        portion = jnp.where(first, code[2:3], 0.0) + jnp.where(second, code[3:4], 0.0)
        scale[:, tile * pitch : (tile + 1) * pitch, :] = jnp.sum(
            portion, axis=1, keepdims=True
        ).reshape(experts, pitch, 1)

    joined = picked.shape[2] // width
    steps = chunks // joined

    def pick(chunk):
        finish(chunk)
        place = chunk % joined * width
        for tile in range(tiles):
            side, start = divmod(tile * per_tile, lines)
            block = tok[chunk, side, start : start + per_tile].reshape(tokens, width)
            found = jnp.dot(hot[tile], block, preferred_element_type=jnp.float32)
            picked[:, tile * pitch : (tile + 1) * pitch, place : place + width] = found.astype(
                jnp.bfloat16
            ).reshape(experts, pitch, width)

    def hidden(step, low, high):
        slot = step % 2

        def one(expert, carry):
            block = picked[expert]
            gate = jnp.dot(block, gate_buf[slot, expert], preferred_element_type=jnp.float32)
            upward = jnp.dot(block, up_buf[slot, expert], preferred_element_type=jnp.float32)
            if step > 0:
                gate = gate + gate_sum[expert]
                upward = upward + up_sum[expert]
            if step + 1 < steps:
                gate_sum[expert] = gate
                up_sum[expert] = upward
            else:
                active[expert] = clamped_unit(gate, upward).astype(jnp.bfloat16)
            return carry

        lax.fori_loop(low, high, one, 0, unroll=2)

    clock = [0]

    def tick():
        now = clock[0]
        clock[0] = now + 1
        for stage, lag in ((pass_line, 0), (pass_side, LAGS[0]), (pass_diag, LAGS[1])):
            if 0 <= now - lag < chunks:
                stage(now - lag)

    def reach(chunk):
        while clock[0] <= min(chunk + LAGS[2], chunks - 1) + LAGS[1]:
            tick()

    for step in range(steps):
        for number in range(joined):
            reach(step * joined + number)
            pick(step * joined + number)
        for copy in weight_copies(step):
            copy.wait()
        hidden(step, 0, experts // 2)
        reach((step + 1) * joined)
        hidden(step, experts // 2, experts)
        if step + 2 < steps:
            for copy in weight_copies(step + 2):
                copy.start()
        if step == 0:
            for later in range(chunks):
                down_copy(later).start()

    for chunk in range(chunks):
        settle(core_land.at[chunk, 0], pass_sem.at[chunk, 0])
        settle(diag_land.at[chunk], pass_sem.at[chunk, 1])
        settle(line_land.at[chunk], pass_sem.at[chunk, 2])
        settle(core_land.at[chunk], pass_sem.at[chunk, 3])

    def lower(chunk):
        down_copy(chunk).wait()

        def one(expert, carry):
            result = jnp.dot(
                active[expert], down_buf[chunk, expert], preferred_element_type=jnp.float32
            )
            picked[expert, :, :width] = (result * scale[expert]).astype(jnp.bfloat16)
            return carry

        lax.fori_loop(0, experts, one, 0, unroll=2)
        for tile in range(tiles):
            block = picked[:, tile * pitch : (tile + 1) * pitch, :width].reshape(span, width)
            total = jnp.dot(hot_turned[tile], block, preferred_element_type=jnp.float32)
            side, start = divmod(tile * per_tile, lines)
            tok[chunk, side, start : start + per_tile] = total.astype(jnp.bfloat16).reshape(
                per_tile, 2, 2, rows, width
            )

    def meet_core(chunk):
        push(
            tok.at[chunk, :, :, :, 1 - core],
            core_land.at[chunk],
            send_back.at[chunk, 0],
            core_back.at[chunk],
            core_device,
        )

    def add(chunk, side, part, up, extra):
        here = (chunk, side, part, up, core)
        tok[here] = (tok[here].astype(jnp.float32) + extra.astype(jnp.float32)).astype(jnp.bfloat16)

    def add_core(chunk, side, part, up):
        add(chunk, side, part, up, core_land[chunk, side, part, up])

    def back_diag(chunk):
        settle(core_land.at[chunk], core_back.at[chunk])
        send = send_back.at[chunk, 1]
        for number, (part, where) in enumerate(((far, y_device), (near, x_device))):
            add_core(chunk, 1 - sp, part, 1 - row)
            push(
                tok.at[chunk, 1 - sp, part, 1 - row, core],
                diag_land.at[chunk, part],
                send,
                diag_back.at[chunk, number],
                where,
            )
        for axis, (part, side, up, where) in enumerate(
            ((near, 1 - sp, row, x_device), (far, sp, 1 - row, y_device))
        ):
            add_core(chunk, side, part, up)
            push(
                tok.at[chunk, side, part, up, core],
                side_land.at[chunk, axis, part],
                send,
                side_back.at[chunk, axis, 0],
                where,
            )
        add_core(chunk, 1 - sp, far, row)
        add_core(chunk, sp, near, 1 - row)
        add_core(chunk, sp, whole, row)

    def back_side(chunk):
        for axis, (part, side, up, where) in enumerate(
            ((far, 1 - sp, row, x_device), (near, sp, 1 - row, y_device))
        ):
            settle(diag_land.at[chunk, part], diag_back.at[chunk, axis])
            add(chunk, side, part, up, diag_land[chunk, part])
            push(
                tok.at[chunk, side, part, up, core],
                side_land.at[chunk, axis, part],
                send_back.at[chunk, 2],
                side_back.at[chunk, axis, 1],
                where,
            )

    def back_line(chunk):
        for axis in range(2):
            for number in range(2):
                settle(side_land.at[chunk, axis, :half], side_back.at[chunk, axis, number])
        own_sum[chunk] = tok[chunk, sp, line, row, core].astype(jnp.float32) + (
            side_land[chunk, 0, line].astype(jnp.float32)
            + side_land[chunk, 1, line].astype(jnp.float32)
        )
        add(
            chunk,
            sp,
            whole,
            row,
            side_land[chunk, 0].astype(jnp.float32) + side_land[chunk, 1].astype(jnp.float32),
        )
        for m in range(1, lines):
            push(
                tok.at[chunk, sp, at_line[m], row, core],
                line_land.at[chunk, m - 1],
                send_back.at[chunk, 3],
                line_back.at[chunk, m - 1],
                line_device[m],
            )

    def close(chunk):
        total = own_sum[chunk]
        for m in range(1, lines):
            settle(line_land.at[chunk, m - 1], line_back.at[chunk, m - 1])
            total = total + line_land[chunk, m - 1].astype(jnp.float32)
        part = slice(chunk * width, (chunk + 1) * width)
        out_ref[:, part] = total

    stages = (back_diag, back_side, back_line, close)
    for step in range(chunks + len(stages)):
        if step < chunks:
            lower(step)
            meet_core(step)
        for number, stage in enumerate(stages):
            chunk = step - 1 - number
            if 0 <= chunk < chunks:
                stage(chunk)
    for chunk in range(chunks):
        settle(core_land.at[chunk], send_back.at[chunk, 0])
        settle(core_land.at[chunk, 0], send_back.at[chunk, 1])
        settle(diag_land.at[chunk], send_back.at[chunk, 2])
        settle(line_land.at[chunk], send_back.at[chunk, 3])


def layer_kernel(pitch, names, attention_count, *refs):
    table = dict(zip(names, refs))
    refs = refs[len(names) :]
    gate_ref, up_ref, down_ref, out_ref, middle_ref = refs[:5]
    refs = refs[5:]
    normed, codes, latents, weights, residual = refs[:5]
    refs = refs[5:]
    held = [name for name in names if name not in PLACED]
    inputs = dict(zip(held, refs))
    refs = refs[len(held) :]
    load_sem, gate_buf, up_buf, weight_sem = refs[:4]
    refs = refs[4:]
    attention_refs, mixture_refs = refs[:attention_count], refs[attention_count:]
    rows = normed.shape[0]
    first_width = table["out_first"].shape[0]
    own_rows = pl.ds(pl.multiple_of(lax.axis_index("tp") * rows, rows), rows)
    width = gate_buf.shape[2]

    def load(number, name):
        source = table[name]
        if name == "latent":
            target = latents.at[0]
        elif name == "out_first":
            target = weights.at[:first_width, :]
        elif name == "out_second":
            target = weights.at[first_width:, :]
        elif name == "residual":
            source, target = source.at[own_rows, :], residual
        else:
            target = inputs[name]
        return pltpu.make_async_copy(source, target, load_sem.at[number])

    loads = {name: load(number, name) for number, name in enumerate(names)}

    def weight_copies(step):
        part = pl.ds(step * width, width)
        slot = step % 2
        return (
            pltpu.make_async_copy(
                gate_ref.at[:, part, :], gate_buf.at[slot], weight_sem.at[slot, 0]
            ),
            pltpu.make_async_copy(up_ref.at[:, part, :], up_buf.at[slot], weight_sem.at[slot, 1]),
        )

    for copy in loads.values():
        copy.start()
    for step in range(2):
        for copy in weight_copies(step):
            copy.start()
    ready = [inputs[name] for name in held]
    (rotaries, queries, state, numerator, *rest) = attention_refs
    attention_kernel(
        pitch,
        *ready,
        loads,
        middle_ref,
        normed,
        codes,
        latents,
        rotaries,
        queries,
        weights,
        residual,
        state,
        numerator,
        *rest,
    )
    tok, hot, hot_turned, scale, picked, gate_sum, up_sum, active, *more = mixture_refs
    mixture_kernel(
        pitch,
        weight_copies,
        normed,
        codes,
        down_ref,
        out_ref,
        tok,
        hot,
        hot_turned,
        scale,
        picked,
        gate_sum,
        up_sum,
        active,
        gate_buf,
        up_buf,
        *more,
    )


PLACED = ("latent", "out_first", "out_second", "residual")
HELD = (
    "table",
    "first",
    "second",
    "rotary",
    "latent_gain",
    "key_first",
    "value_first",
    "key_second",
    "value_second",
    "expert_gain",
    "routes",
    "scores",
)


def run_layer(named, gate_weight, up_weight, down_weight, rows, pitch, collective_id):
    groups, sets = lax.axis_size("sp"), lax.axis_size("tp")
    lines = sets // 4
    seq_rows, rank = named["latent"].shape
    experts, depth, units = gate_weight.shape
    width, joint = depth // CHUNKS, depth // JOINT
    strip = depth // STRIPS
    first, second, rotary = named["first"], named["second"], named["rotary"]
    heads = named["out_first"].shape[0] + named["out_second"].shape[0]
    tiles = groups * sets * rows // TILE_TOKENS
    span = experts * pitch
    slots = tiles * pitch
    narrow, wide = jnp.bfloat16, jnp.float32
    anywhere = pl.BlockSpec(memory_space=pl.ANY)
    dma, keep = pltpu.SemaphoreType.DMA, pltpu.VMEM
    attention = [
        keep(rotary.shape, narrow),
        keep((first.shape[0] + second.shape[0], seq_rows), narrow),
        keep((8, seq_rows), wide),
        keep((heads, seq_rows), wide),
        keep((STRIPS, lines, 2, 2, rows, strip), narrow),
        keep((STRIPS, lines, 2, rows, strip), narrow),
        keep((STRIPS, lines, rows, strip), narrow),
        keep((STRIPS, lines - 1, rows, strip), narrow),
        keep((STRIPS, rows, strip), wide),
        dma((4,)),
        dma((3,)),
        dma((STRIPS,)),
        dma((STRIPS,)),
        dma((STRIPS, lines - 1)),
        dma((STRIPS, 3)),
    ]
    mixture = [
        keep((CHUNKS, groups, lines, 2, 2, rows, width), narrow),
        keep((tiles, span, TILE_TOKENS), narrow),
        keep((tiles, TILE_TOKENS, span), narrow),
        keep((experts, slots, 1), wide),
        keep((experts, slots, joint), narrow),
        keep((experts, slots, units), wide),
        keep((experts, slots, units), wide),
        keep((experts, slots, units), narrow),
        keep((CHUNKS, experts, units, width), narrow),
        keep((CHUNKS, groups, lines, 2, rows, width), narrow),
        keep((CHUNKS, lines, rows, width), narrow),
        keep((CHUNKS, 2, lines, rows, width), narrow),
        keep((CHUNKS, lines - 1, rows, width), narrow),
        keep((CHUNKS, rows, width), wide),
        dma((CHUNKS, lines - 1)),
        dma((CHUNKS, 2, lines // 2 + 1)),
        dma((CHUNKS, 2)),
        dma((CHUNKS, 4)),
        dma((CHUNKS, 4)),
        dma((CHUNKS,)),
        dma((CHUNKS, 2)),
        dma((CHUNKS, 2, 2)),
        dma((CHUNKS, lines - 1)),
        dma((CHUNKS, 4)),
        dma((CHUNKS,)),
    ]
    names = HELD + PLACED
    shared = [
        keep((rows, depth), narrow),
        keep((groups, 8, seq_rows), wide),
        keep((2, seq_rows, rank), narrow),
        keep((heads, depth), narrow),
        keep((rows, depth), narrow),
        *[keep(named[name].shape, named[name].dtype) for name in HELD],
        dma((len(names),)),
        keep((2, experts, joint, units), narrow),
        keep((2, experts, joint, units), narrow),
        dma((2, 2)),
    ]
    return pl.pallas_call(
        functools.partial(layer_kernel, pitch, names, len(attention)),
        out_shape=(
            jax.ShapeDtypeStruct((rows, depth), wide),
            jax.ShapeDtypeStruct((rows, depth), narrow),
        ),
        in_specs=[anywhere] * (len(names) + 3),
        out_specs=(VMEM, VMEM),
        scratch_shapes=shared + attention + mixture,
        compiler_params=pltpu.CompilerParams(
            collective_id=collective_id, has_side_effects=True, vmem_limit_bytes=63 << 20
        ),
        name="run_layer",
    )(*[named[name] for name in names], gate_weight, up_weight, down_weight)


def token_body(
    query_first,
    query_second,
    latent,
    key_rotary,
    latent_gain,
    key_up_first,
    value_up_first,
    key_up_second,
    value_up_second,
    out_first,
    out_second,
    residual,
    expert_gain,
    route_experts,
    route_scores,
    gate_weight,
    up_weight,
    down_weight,
):
    seq_rows = latent.shape[0]
    sets = lax.axis_size("tp")
    groups = lax.axis_size("sp")
    own_rows = seq_rows // sets
    span_blocks = TILE_TOKENS // own_rows
    pitch = -(-span_blocks * CAP // 16) * 16
    half = key_rotary.shape[1] // 2
    inverse = np.float32(rotary_base) ** (-np.arange(half, dtype=np.float32) / half)
    angles = inverse[:, None] * np.arange(groups * seq_rows, dtype=np.float32)[None, :]
    table = np.concatenate([np.cos(angles), np.sin(angles)], axis=0).astype(np.float32)
    named = {
        "table": jnp.asarray(table),
        "first": query_first.T,
        "second": query_second.T,
        "latent": latent,
        "rotary": key_rotary.T,
        "latent_gain": latent_gain[None, :],
        "key_first": key_up_first.T,
        "value_first": value_up_first.T,
        "key_second": key_up_second,
        "value_second": value_up_second,
        "out_first": out_first,
        "out_second": out_second,
        "residual": residual,
        "expert_gain": expert_gain[None, :],
        "routes": route_experts.T,
        "scores": route_scores.T,
    }
    mixture, middle = run_layer(
        named, gate_weight, up_weight, down_weight, own_rows, pitch, 0
    )
    return (middle.astype(jnp.float32) + mixture).astype(jnp.bfloat16)


def solution(mesh):
    in_specs = (
        P("sp", "tp"),
        P("sp", "tp"),
        P("sp", None),
        P("sp", None),
        P(),
        P(None, "tp"),
        P(None, "tp"),
        P(None, "tp"),
        P(None, "tp"),
        P("tp", None),
        P("tp", None),
        P("sp", None),
        P(),
        P("sp", None),
        P("sp", None),
        P("sp", None, "tp"),
        P("sp", None, "tp"),
        P("sp", "tp", None),
    )
    out_specs = P(("sp", "tp"), None)
    groups, sets = mesh.shape["sp"], mesh.shape["tp"]
    small = groups == 2 and sets & (sets - 1) == 0 and sets > 4

    def body(*arguments):
        fits = small and arguments[2].shape[0] * groups <= 1024
        return (token_body if fits else slot_body)(*arguments)

    return jax.shard_map(body, mesh=mesh, in_specs=in_specs, out_specs=out_specs, check_vma=False)
```

```python
import functools

import jax
import jax.numpy as jnp
import numpy as np
from jax import lax
from jax.experimental import pallas as pl
from jax.experimental.pallas import tpu as pltpu
from jax.sharding import PartitionSpec as P

NA = 64
NB = 128
ROPE = 32
CAP = 3


norm_epsilon = 1e-06
rotary_base = 10000.0
clamp_limit = 7.0
sigmoid_slope = 1.702
masked_score = -1e30


def rotate(values, positions):
    half = values.shape[-1] // 2
    inverse = rotary_base ** (-jnp.arange(half, dtype=jnp.float32) / half)
    angles = positions.astype(jnp.float32)[:, None, None] * inverse[None, None, :]
    cosine = jnp.cos(angles)
    sine = jnp.sin(angles)
    first = values[..., :half]
    second = values[..., half:]
    return jnp.concatenate(
        [first * cosine - second * sine, second * cosine + first * sine], axis=-1
    )


def rms_scaled(values, gain):
    wide = values.astype(jnp.float32)
    return wide * lax.rsqrt(jnp.mean(wide * wide, axis=-1, keepdims=True) + norm_epsilon) * gain


def turned_queries(query, nope, positions):
    shaped = query.reshape(query.shape[0], query.shape[1] // (nope + ROPE), nope + ROPE)
    turned = rotate(shaped[..., nope:].astype(jnp.float32), positions).astype(jnp.bfloat16)
    return jnp.concatenate([shaped[..., :nope], turned], axis=-1)


def clamped_unit(gate, upward):
    limited = jnp.minimum(gate, clamp_limit)
    bounded = jnp.clip(upward, -clamp_limit, clamp_limit)
    return (bounded + 1.0) * limited * jax.nn.sigmoid(sigmoid_slope * limited)


def slot_numbers(chosen, experts):
    hits = (chosen[..., None] == jnp.arange(experts, dtype=jnp.int32)).astype(jnp.int32)
    before = jnp.cumsum(hits, axis=-2) - hits
    return chosen * CAP + jnp.sum(before * hits, axis=-1)


def fold_group(state, queries, key_nope, key_turned, values, query_places, scale):
    running, denominator, numerator = state
    heads = queries.shape[1]
    nope = queries.shape[2] - key_turned.shape[1]
    keys = key_nope.reshape(key_nope.shape[0], heads, nope)
    value_rows = values.reshape(values.shape[0], heads, values.shape[1] // heads)
    score = jnp.einsum(
        "qhd,khd->qhk", queries[..., :nope], keys, preferred_element_type=jnp.float32
    )
    score = score + jnp.einsum(
        "qhr,kr->qhk", queries[..., nope:], key_turned, preferred_element_type=jnp.float32
    )
    score = score * scale
    key_places = jnp.arange(keys.shape[0], dtype=jnp.int32)
    allowed = (query_places[:, None] >= key_places[None, :])[:, None, :]
    score = jnp.where(allowed, score, masked_score)
    highest = jnp.maximum(running, jnp.max(score, axis=-1))
    weights = jnp.where(allowed, jnp.exp(score - highest[..., None]), 0.0)
    denominator = jnp.sum(weights, axis=-1)
    numerator = jnp.einsum(
        "qhk,khd->qhd", weights.astype(jnp.bfloat16), value_rows, preferred_element_type=jnp.float32
    )
    return (highest, denominator, numerator)


def expert_hidden(rows, gate_weight, up_weight):
    gate = jnp.einsum("nsecd,edf->nsecf", rows, gate_weight, preferred_element_type=jnp.float32)
    upward = jnp.einsum("nsecd,edf->nsecf", rows, up_weight, preferred_element_type=jnp.float32)
    return clamped_unit(gate, upward).astype(jnp.bfloat16)


def slot_body(
    query_first,
    query_second,
    latent,
    key_rotary,
    latent_gain,
    key_up_first,
    value_up_first,
    key_up_second,
    value_up_second,
    out_first,
    out_second,
    residual,
    expert_gain,
    route_experts,
    route_scores,
    gate_weight,
    up_weight,
    down_weight,
):
    seq_rows = latent.shape[0]
    sets = lax.axis_size("tp")
    groups = lax.axis_size("sp")
    own_rows = seq_rows // sets
    topk = route_experts.shape[1]
    local_experts = gate_weight.shape[0]
    experts = local_experts * groups
    offset = lax.axis_index("sp") * seq_rows
    places = offset + jnp.arange(seq_rows, dtype=jnp.int32)
    last_place = offset + seq_rows - 1
    queries_first = turned_queries(query_first, NA, places)
    queries_second = turned_queries(query_second, NB, places)
    key_turned = rotate(key_rotary.astype(jnp.float32)[:, None, :], places)[:, 0, :].astype(
        jnp.bfloat16
    )
    latent_normed = rms_scaled(latent, latent_gain).astype(jnp.bfloat16)
    scale_first = (NA + ROPE) ** (-0.5)
    scale_second = (NB + ROPE) ** (-0.5)

    def attend(carry, parts):
        key_first, value_first, key_second, value_second, turned = parts
        return (
            fold_group(
                carry[0], queries_first, key_first, turned, value_first, places, scale_first
            ),
            fold_group(
                carry[1], queries_second, key_second, turned, value_second, places, scale_second
            ),
        )

    def initial(queries, value_width):
        shape = queries.shape[:2]
        return (
            jnp.full(shape, masked_score, jnp.float32),
            jnp.zeros(shape, jnp.float32),
            jnp.zeros(shape + (value_width,), jnp.float32),
        )

    start_state = (
        initial(queries_first, value_up_first.shape[1] // queries_first.shape[1]),
        initial(queries_second, value_up_second.shape[1] // queries_second.shape[1]),
    )
    key_first, value_first, key_second, value_second = tuple(
        (
            jnp.dot(latent_normed, weight, preferred_element_type=jnp.float32).astype(jnp.bfloat16)
            for weight in (key_up_first, value_up_first, key_up_second, value_up_second)
        )
    )
    parts = (
        lax.all_gather(key_first, "sp", axis=0, tiled=True),
        lax.all_gather(value_first, "sp", axis=0, tiled=True),
        lax.all_gather(key_second, "sp", axis=0, tiled=True),
        lax.all_gather(value_second, "sp", axis=0, tiled=True),
        lax.all_gather(key_turned, "sp", axis=0, tiled=True),
    )
    state = lax.cond(
        jnp.int32(0) <= last_place,
        lambda inner: attend(inner, parts),
        lambda inner: inner,
        start_state,
    )
    first_state, second_state = state
    attended_first = (
        (first_state[2] / first_state[1][..., None]).astype(jnp.bfloat16).reshape(seq_rows, -1)
    )
    attended_second = (
        (second_state[2] / second_state[1][..., None]).astype(jnp.bfloat16).reshape(seq_rows, -1)
    )
    own_start = lax.axis_index("tp") * own_rows
    slot_range = jnp.arange(experts * CAP, dtype=jnp.int32)
    projected = lax.psum_scatter(
        (
            jnp.dot(attended_first, out_first, preferred_element_type=jnp.float32)
            + jnp.dot(attended_second, out_second, preferred_element_type=jnp.float32)
        ).astype(jnp.bfloat16),
        "tp",
        scatter_dimension=0,
        tiled=True,
    ).astype(jnp.float32)
    own_residual = lax.dynamic_slice_in_dim(residual, own_start, own_rows, 0)
    middle = (own_residual.astype(jnp.float32) + projected).astype(jnp.bfloat16)
    normed = rms_scaled(middle, expert_gain).astype(jnp.bfloat16)
    own_ids = lax.dynamic_slice_in_dim(route_experts, own_start, own_rows, 0).reshape(-1)
    own_slots = slot_numbers(own_ids, experts)
    picks = (own_slots[:, None] == slot_range).reshape(own_rows, topk, experts * CAP)
    selected = jnp.sum(picks.astype(jnp.float32), axis=1).astype(jnp.bfloat16)
    outgoing = jnp.einsum("ts,td->sd", selected, normed, preferred_element_type=jnp.float32).astype(
        jnp.bfloat16
    )
    outgoing = outgoing.reshape(groups, local_experts, CAP, outgoing.shape[-1])
    arrived = lax.all_to_all(outgoing, "sp", split_axis=0, concat_axis=0, tiled=True)
    activated = expert_hidden(
        lax.all_gather(arrived[None], "tp", axis=0, tiled=True), gate_weight, up_weight
    )
    flat_hidden = activated.reshape(sets * groups, local_experts, CAP, activated.shape[-1])
    summed = lax.psum_scatter(
        jnp.einsum(
            "secf,efd->secd", flat_hidden, down_weight, preferred_element_type=jnp.float32
        ).astype(jnp.bfloat16),
        "tp",
        scatter_dimension=0,
        tiled=True,
    )
    returned = lax.all_to_all(summed, "sp", split_axis=0, concat_axis=0, tiled=True)
    expert_out = returned.reshape(experts * CAP, returned.shape[-1]).astype(jnp.float32)
    own_scores = lax.dynamic_slice_in_dim(route_scores, own_start, own_rows, 0)
    route_weight = jax.nn.softmax(own_scores, axis=-1)
    matches = own_slots.reshape(own_rows, topk)[..., None] == slot_range
    combine = jnp.sum(jnp.where(matches, route_weight[..., None], 0.0), axis=1)
    mixture = jnp.dot(combine, expert_out, precision=lax.Precision.HIGHEST)
    return (middle.astype(jnp.float32) + mixture).astype(jnp.bfloat16)


MESH = pl.DeviceIdType.MESH
VMEM = pl.BlockSpec(memory_space=pltpu.VMEM)
TILE_TOKENS = 256
CHUNKS = 4
JOINT = 4
STRIPS = 4
EARLY = 2
ORDER = (
    "L0", "O2", "L1", "S0", "O3", "L2", "D0", "S1", "P0", "L3", "A0", "D1", "S2", "B0", "P1",
    "A1", "D2", "S3", "B1", "P2", "A2", "D3", "B2", "P3", "A3", "B3",
)
PIECES = 2


def flipped(value, mask, bits):
    total = 0
    for bit in range(bits):
        digit = (value // (1 << bit)) % 2
        total = total + (1 << bit) * (1 - digit if mask >> bit & 1 else digit)
    return total


def attention_kernel(
    pitch,
    table_ref,
    first_ref,
    second_ref,
    rotary_ref,
    latent_gain_ref,
    key_first_ref,
    value_first_ref,
    key_second_ref,
    value_second_ref,
    expert_gain_ref,
    route_ref,
    score_ref,
    loads,
    middle_ref,
    normed_ref,
    codes_ref,
    latents,
    rotaries,
    queries,
    weights,
    residual,
    state,
    numerator,
    part,
    core_land,
    side_land,
    line_land,
    total,
    cross_sem,
    cross_back,
    core_sem,
    side_sem,
    line_sem,
    send_sem,
):
    sets = lax.axis_size("tp")
    lines = sets // 4
    bits = lines.bit_length() - 1
    chunks, _, _, _, rows, width = part.shape
    _, seq_rows, rank = latents.shape
    first_nope, second_nope = key_first_ref.shape[0], key_second_ref.shape[1]
    first_width, second_width = value_first_ref.shape[0], value_second_ref.shape[1]
    half_turn = table_ref.shape[0] // 2
    rotary = 2 * half_turn
    sp, tp = lax.axis_index("sp"), lax.axis_index("tp")
    core, row, line = tp % 2, (tp // 2) % 2, tp // 4
    wide, narrow = jnp.float32, jnp.bfloat16

    at_line = [flipped(line, m, bits) for m in range(lines)]
    x_device = {"sp": 1 - sp, "tp": tp}
    y_device = {"sp": sp, "tp": line * 4 + (1 - row) * 2 + core}
    core_device = {"sp": sp, "tp": line * 4 + row * 2 + 1 - core}
    line_device = [{"sp": sp, "tp": at_line[m] * 4 + row * 2 + core} for m in range(lines)]

    barrier = pltpu.get_barrier_semaphore()
    everyone = [x_device, y_device, core_device] + line_device[1:]
    for one in everyone:
        pl.semaphore_signal(barrier, inc=1, device_id=one, device_id_type=MESH)

    def push(source, target, send, receive, where):
        copy = pltpu.make_async_remote_copy(
            src_ref=source,
            dst_ref=target,
            send_sem=send,
            recv_sem=receive,
            device_id=where,
            device_id_type=MESH,
        )
        copy.start()
        return copy

    def settle(view, sem):
        pltpu.make_async_copy(view, view, sem).wait()

    some = seq_rows // (2 * PIECES)
    mine = pl.ds(pl.multiple_of(core * (seq_rows // 2), seq_rows // 2), seq_rows // 2)

    def piece(side, number):
        return pl.ds(pl.multiple_of((side * PIECES + number) * some, some), some)

    loads["latent"].wait()
    loads["rotary"].wait()
    pl.semaphore_wait(barrier, len(everyone))

    @pl.when(sp == 0)
    def _():
        push(rotary_ref, rotaries, cross_back.at[1], cross_sem.at[1], x_device)
        for number in range(PIECES):
            here = piece(core, number)
            push(
                latents.at[0, here, :],
                latents.at[1, here, :],
                cross_back.at[0],
                cross_sem.at[3 + number],
                x_device,
            )

    for name in ("routes", "scores"):
        loads[name].wait()

    tile = 4 * rows
    own_codes = codes_ref.at[sp]
    scores = score_ref[...]
    raised = jnp.exp(scores - jnp.max(scores, axis=0, keepdims=True))
    shares = raised / jnp.sum(raised, axis=0, keepdims=True)
    chosen = route_ref[...].astype(wide)
    upright = jnp.concatenate([chosen] * 4, axis=0).T
    earlier = lax.broadcasted_iota(jnp.int32, (tile, tile), 0)
    later = lax.broadcasted_iota(jnp.int32, (tile, tile), 1)
    counted = (earlier < later) & (earlier // rows == later // rows)
    places = lax.broadcasted_iota(jnp.int32, (1, seq_rows), 1)
    span_blocks = TILE_TOKENS // rows
    spots = (places // rows % span_blocks * CAP).astype(wide)
    lists = []
    for choice in range(2):
        ranks = []
        for start in range(0, seq_rows, tile):
            wanted = chosen[choice : choice + 1, start : start + tile]
            same = (upright[start : start + tile, 0:1] == wanted) | (
                upright[start : start + tile, 1:2] == wanted
            )
            ranks.append(jnp.sum(jnp.where(same & counted, 1.0, 0.0), axis=0, keepdims=True))
        lists.append(
            chosen[choice : choice + 1] * pitch + spots + jnp.concatenate(ranks, axis=1)
        )
    lists = jnp.concatenate(lists + [shares], axis=0)
    own_codes[...] = jnp.concatenate([lists, lists], axis=0)
    route_copy = push(own_codes, own_codes, cross_back.at[2], cross_sem.at[2], x_device)

    for name in (
        "table",
        "first",
        "second",
        "latent_gain",
        "key_first",
        "value_first",
        "key_second",
        "value_second",
    ):
        loads[name].wait()
    own_places = pl.ds(pl.multiple_of(sp * seq_rows, seq_rows), seq_rows)

    def turned(values, where):
        cosine, sine = table_ref[:half_turn, where], table_ref[half_turn:, where]
        upper, lower = values[:half_turn].astype(wide), values[half_turn:].astype(wide)
        return jnp.concatenate(
            [upper * cosine - lower * sine, lower * cosine + upper * sine], axis=0
        )

    first_end = first_nope + rotary
    queries[:first_nope] = first_ref[:first_nope]
    queries[first_nope:first_end] = turned(first_ref[first_nope:], own_places).astype(narrow)
    queries[first_end : first_end + second_nope] = second_ref[:second_nope]
    queries[first_end + second_nope :] = turned(second_ref[second_nope:], own_places).astype(narrow)
    value_second = value_second_ref[...].astype(wide).T.astype(narrow)
    across = (((1,), (1,)), ((), ()))

    def fold(slot, span, rotary_values, where, causal, fresh):
        raw = latents[slot, span, :].astype(wide)
        root = lax.rsqrt(jnp.mean(raw * raw, axis=-1, keepdims=True) + norm_epsilon)
        base = (raw * root * latent_gain_ref[...]).astype(narrow)
        turned_keys = turned(rotary_values, where).T.astype(narrow)
        if causal:
            key_places = lax.broadcasted_iota(jnp.int32, (seq_rows, seq_rows), 0)
            query_places = lax.broadcasted_iota(jnp.int32, (seq_rows, seq_rows), 1)
            allowed = key_places <= query_places
        for group in range(2):
            if group == 0:
                keys = lax.dot_general(base, key_first_ref[...], across, preferred_element_type=wide)
                values = lax.dot_general(
                    value_first_ref[...], base, across, preferred_element_type=wide
                )
                found = queries[:first_end]
                spots = pl.ds(0, first_width)
            else:
                keys = jnp.dot(base, key_second_ref[...], preferred_element_type=wide)
                values = lax.dot_general(value_second, base, across, preferred_element_type=wide)
                found = queries[first_end:]
                spots = pl.ds(first_width, second_width)
            keys = jnp.concatenate([keys.astype(narrow), turned_keys], axis=1)
            score = jnp.dot(keys, found, preferred_element_type=wide) * (
                keys.shape[1] ** (-0.5)
            )
            if causal:
                score = jnp.where(allowed, score, masked_score)
            highest = jnp.max(score, axis=0, keepdims=True)
            if not fresh:
                before = state[group : group + 1]
                highest = jnp.maximum(highest, before)
                kept = jnp.exp(before - highest)
            raised = jnp.exp(score - highest)
            amount = jnp.sum(raised, axis=0, keepdims=True)
            mixed = jnp.dot(
                values.astype(narrow), raised.astype(narrow), preferred_element_type=wide
            )
            if not fresh:
                amount = amount + kept * state[group + 2 : group + 3]
                mixed = mixed + kept * numerator[spots, :]
            state[group : group + 1] = highest
            state[group + 2 : group + 3] = amount
            numerator[spots, :] = mixed

    fold(0, slice(None), rotary_ref[...], own_places, True, True)

    @pl.when(sp == 1)
    def _():
        settle(rotaries, cross_sem.at[1])
        for number in range(PIECES):
            here = piece(core, number)
            there = latents.at[1, here, :]
            settle(there, cross_sem.at[3 + number])
            push(there, there, cross_back.at[0], cross_sem.at[3 + PIECES + number], core_device)
            fold(1, here, rotaries[:, here], here, False, False)
            here = piece(1 - core, number)
            settle(latents.at[1, here, :], cross_sem.at[3 + PIECES + number])
            fold(1, here, rotaries[:, here], here, False, False)
        settle(latents.at[1, mine, :], cross_back.at[0])

    @pl.when(sp == 0)
    def _():
        settle(latents.at[0, mine, :], cross_back.at[0])
        settle(rotary_ref, cross_back.at[1])

    attended = jnp.concatenate(
        [
            numerator[:first_width] / state[2:3],
            numerator[first_width:] / state[3:4],
        ],
        axis=0,
    )
    attended = attended.T.astype(narrow)
    for name in ("out_first", "out_second", "residual", "expert_gain"):
        loads[name].wait()

    def project(chunk):
        columns = slice(chunk * width, (chunk + 1) * width)
        found = jnp.dot(attended, weights[:, columns], preferred_element_type=wide)
        part[chunk] = found.astype(narrow).reshape(lines, 2, 2, rows, width)
        push(
            part.at[chunk, :, :, 1 - core],
            core_land.at[chunk],
            send_sem.at[chunk, 0],
            core_sem.at[chunk],
            core_device,
        )

    def add_core(chunk, up):
        part[chunk, :, up, core] = (
            part[chunk, :, up, core].astype(wide) + core_land[chunk, :, up].astype(wide)
        ).astype(narrow)

    def to_side(chunk):
        settle(core_land.at[chunk], core_sem.at[chunk])
        add_core(chunk, 1 - row)
        push(
            part.at[chunk, :, 1 - row, core],
            side_land.at[chunk],
            send_sem.at[chunk, 1],
            side_sem.at[chunk],
            y_device,
        )
        add_core(chunk, row)

    def to_line(chunk):
        settle(side_land.at[chunk], side_sem.at[chunk])
        total[chunk] = part[chunk, line, row, core].astype(wide) + side_land[chunk, line].astype(
            wide
        )
        part[chunk, :, row, core] = (
            part[chunk, :, row, core].astype(wide) + side_land[chunk].astype(wide)
        ).astype(narrow)
        for m in range(lines - 1, 0, -1):
            push(
                part.at[chunk, at_line[m], row, core],
                line_land.at[chunk, m - 1],
                send_sem.at[chunk, 2],
                line_sem.at[chunk, m - 1],
                line_device[m],
            )

    def close(chunk):
        value = total[chunk]
        for m in range(1, lines):
            settle(line_land.at[chunk, m - 1], line_sem.at[chunk, m - 1])
            value = value + line_land[chunk, m - 1].astype(wide)
        columns = slice(chunk * width, (chunk + 1) * width)
        middle_ref[:, columns] = (residual[:, columns].astype(wide) + value).astype(narrow)

    stages = (to_side, to_line, close)
    for stage in (project, *stages):
        for chunk in range(chunks):
            stage(chunk)
    middle = middle_ref[...].astype(wide)
    root = lax.rsqrt(jnp.mean(middle * middle, axis=-1, keepdims=True) + norm_epsilon)
    normed_ref[...] = (middle * root * expert_gain_ref[...]).astype(narrow)
    for chunk in range(chunks):
        settle(core_land.at[chunk], send_sem.at[chunk, 0])
        settle(side_land.at[chunk], send_sem.at[chunk, 1])
        settle(line_land.at[chunk], send_sem.at[chunk, 2])
    route_copy.wait_send()
    settle(codes_ref.at[0], cross_sem.at[2])


def mixture_kernel(
    pitch,
    weight_copies,
    x_ref,
    code_ref,
    down_ref,
    out_ref,
    tok,
    hot,
    hot_turned,
    scale,
    picked,
    gate_sum,
    up_sum,
    active,
    gate_buf,
    up_buf,
    down_buf,
    core_land,
    diag_land,
    side_land,
    line_land,
    own_sum,
    line_sem,
    side_sem,
    diag_sem,
    core_sem,
    pass_sem,
    core_back,
    diag_back,
    side_back,
    line_back,
    send_back,
    down_sem,
):
    groups, sets = lax.axis_size("sp"), lax.axis_size("tp")
    lines = sets // 4
    bits = lines.bit_length() - 1
    chunks, _, _, _, _, rows, width = tok.shape
    experts = picked.shape[0]
    tiles, span, tokens = hot.shape
    per_tile = tokens // (4 * rows)
    half = lines // 2
    sp, tp = lax.axis_index("sp"), lax.axis_index("tp")
    core, row, line = tp % 2, (tp // 2) % 2, tp // 4

    def device(side, at, up, half_chip):
        return {"sp": side, "tp": at * 4 + up * 2 + half_chip}

    at_line = [flipped(line, m, bits) for m in range(lines)]
    high = line // half
    near = pl.ds(high * half, half)
    far = pl.ds((1 - high) * half, half)
    whole = slice(None)
    x_device = device(1 - sp, line, row, core)
    y_device = device(sp, line, 1 - row, core)
    core_device = device(sp, line, row, 1 - core)
    line_device = [device(sp, at_line[m], row, core) for m in range(lines)]

    def down_copy(chunk):
        part = pl.ds(chunk * width, width)
        return pltpu.make_async_copy(
            down_ref.at[:, :, part], down_buf.at[chunk], down_sem.at[chunk]
        )

    def push(source, target, send, receive, where):
        pltpu.make_async_remote_copy(
            src_ref=source,
            dst_ref=target,
            send_sem=send,
            recv_sem=receive,
            device_id=where,
            device_id_type=MESH,
        ).start()

    def settle(view, sem):
        pltpu.make_async_copy(view, view, sem).wait()

    def share(chunk, side, up, number):
        column = tok.at[chunk, side, :, up, core]
        push(column, column, pass_sem.at[chunk, 3], core_sem.at[chunk, number], core_device)

    def send_own(chunk):
        source = x_ref.at[:, pl.ds(chunk * width, width)]
        target = tok.at[chunk, sp, line, row, core]
        for m in range(lines - 1, 0, -1):
            push(source, target, pass_sem.at[chunk, 2], line_sem.at[chunk, m - 1], line_device[m])
        push(source, target, pass_sem.at[chunk, 0], side_sem.at[chunk, 0, 0], x_device)
        push(source, target, pass_sem.at[chunk, 0], side_sem.at[chunk, 1, 0], y_device)

    def pass_line(chunk):
        def onward(here, number):
            early = pass_sem.at[chunk, 0]
            push(here, here, early, side_sem.at[chunk, 0, number], x_device)
            push(here, here, early, side_sem.at[chunk, 1, number], y_device)

        for m in range(1, lines):
            here = tok.at[chunk, sp, at_line[m], row, core]
            settle(here, line_sem.at[chunk, m - 1])
            if m < half:
                onward(here, m)
        onward(tok.at[chunk, sp, far, row, core], half)
        share(chunk, sp, row, 0)

    def settle_near(chunk, axis, side, up):
        for m in range(half):
            settle(tok.at[chunk, side, at_line[m], up, core], side_sem.at[chunk, axis, m])

    def pass_side(chunk):
        by_x, by_y = (chunk, 1 - sp), (chunk, sp)
        late = pass_sem.at[chunk, 1]
        settle_near(chunk, 1, sp, 1 - row)
        here = tok.at[(*by_y, near, 1 - row, core)]
        push(here, here, late, diag_sem.at[chunk, 1], x_device)
        here = tok.at[(*by_x, far, row, core)]
        settle(here, side_sem.at[chunk, 0, half])
        push(here, here, late, diag_sem.at[chunk, 0], y_device)
        settle_near(chunk, 0, 1 - sp, row)
        share(chunk, 1 - sp, row, 1)
        settle(tok.at[(*by_y, far, 1 - row, core)], side_sem.at[chunk, 1, half])
        share(chunk, sp, 1 - row, 2)

    def pass_diag(chunk):
        for number, part in enumerate((far, near)):
            settle(tok.at[chunk, 1 - sp, part, 1 - row, core], diag_sem.at[chunk, number])
        share(chunk, 1 - sp, 1 - row, 3)

    def finish(chunk):
        for number in range(4):
            settle(tok.at[chunk, 0, :, 0, 0], core_sem.at[chunk, number])

    for chunk in range(EARLY):
        send_own(chunk)
    for chunk in range(chunks):
        tok[chunk, sp, line, row, core] = x_ref[:, chunk * width : (chunk + 1) * width]

    for tile in range(tiles):
        slots = lax.broadcasted_iota(jnp.int32, (span, tokens), 0)
        side, place = divmod(tile * tokens, code_ref.shape[2])
        code = code_ref[side, :, place : place + tokens]
        slots = slots + sp * span
        first = slots == code[0:1].astype(jnp.int32)
        second = slots == code[1:2].astype(jnp.int32)
        chosen = jnp.where(first | second, 1.0, 0.0)
        hot[tile] = chosen.astype(jnp.bfloat16)
        hot_turned[tile] = chosen.T.astype(jnp.bfloat16)
        portion = jnp.where(first, code[2:3], 0.0) + jnp.where(second, code[3:4], 0.0)
        scale[:, tile * pitch : (tile + 1) * pitch, :] = jnp.sum(
            portion, axis=1, keepdims=True
        ).reshape(experts, pitch, 1)

    joined = picked.shape[2] // width
    steps = chunks // joined

    def pick(chunk):
        finish(chunk)
        place = chunk % joined * width
        for tile in range(tiles):
            side, start = divmod(tile * per_tile, lines)
            block = tok[chunk, side, start : start + per_tile].reshape(tokens, width)
            found = jnp.dot(hot[tile], block, preferred_element_type=jnp.float32)
            picked[:, tile * pitch : (tile + 1) * pitch, place : place + width] = found.astype(
                jnp.bfloat16
            ).reshape(experts, pitch, width)

    def hidden(step, low, high):
        slot = step % 2

        def one(expert, carry):
            block = picked[expert]
            gate = jnp.dot(block, gate_buf[slot, expert], preferred_element_type=jnp.float32)
            upward = jnp.dot(block, up_buf[slot, expert], preferred_element_type=jnp.float32)
            if step > 0:
                gate = gate + gate_sum[expert]
                upward = upward + up_sum[expert]
            if step + 1 < steps:
                gate_sum[expert] = gate
                up_sum[expert] = upward
            else:
                active[expert] = clamped_unit(gate, upward).astype(jnp.bfloat16)
            return carry

        lax.fori_loop(low, high, one, 0, unroll=2)

    def first_half(step):
        for copy in weight_copies(step):
            copy.wait()
        hidden(step, 0, experts // 2)

    def second_half(step):
        hidden(step, experts // 2, experts)
        if step + 2 < steps:
            for copy in weight_copies(step + 2):
                copy.start()
        if step == 0:
            for later in range(chunks):
                down_copy(later).start()

    moves = {
        "O": send_own,
        "L": pass_line,
        "S": pass_side,
        "D": pass_diag,
        "P": pick,
        "A": first_half,
        "B": second_half,
    }
    for move in ORDER:
        moves[move[0]](int(move[1:]))

    for chunk in range(chunks):
        settle(core_land.at[chunk, 0], pass_sem.at[chunk, 0])
        settle(diag_land.at[chunk], pass_sem.at[chunk, 1])
        settle(line_land.at[chunk], pass_sem.at[chunk, 2])
        settle(core_land.at[chunk], pass_sem.at[chunk, 3])

    def lower(chunk):
        down_copy(chunk).wait()

        def one(expert, carry):
            result = jnp.dot(
                active[expert], down_buf[chunk, expert], preferred_element_type=jnp.float32
            )
            picked[expert, :, :width] = (result * scale[expert]).astype(jnp.bfloat16)
            return carry

        lax.fori_loop(0, experts, one, 0, unroll=2)
        for tile in range(tiles):
            block = picked[:, tile * pitch : (tile + 1) * pitch, :width].reshape(span, width)
            total = jnp.dot(hot_turned[tile], block, preferred_element_type=jnp.float32)
            side, start = divmod(tile * per_tile, lines)
            tok[chunk, side, start : start + per_tile] = total.astype(jnp.bfloat16).reshape(
                per_tile, 2, 2, rows, width
            )

    def meet_core(chunk):
        push(
            tok.at[chunk, :, :, :, 1 - core],
            core_land.at[chunk],
            send_back.at[chunk, 0],
            core_back.at[chunk],
            core_device,
        )

    def add(chunk, side, part, up, extra):
        here = (chunk, side, part, up, core)
        tok[here] = (tok[here].astype(jnp.float32) + extra.astype(jnp.float32)).astype(jnp.bfloat16)

    def add_core(chunk, side, part, up):
        add(chunk, side, part, up, core_land[chunk, side, part, up])

    def back_diag(chunk):
        settle(core_land.at[chunk], core_back.at[chunk])
        send = send_back.at[chunk, 1]
        for number, (part, where) in enumerate(((far, y_device), (near, x_device))):
            add_core(chunk, 1 - sp, part, 1 - row)
            push(
                tok.at[chunk, 1 - sp, part, 1 - row, core],
                diag_land.at[chunk, part],
                send,
                diag_back.at[chunk, number],
                where,
            )
        for axis, (part, side, up, where) in enumerate(
            ((near, 1 - sp, row, x_device), (far, sp, 1 - row, y_device))
        ):
            add_core(chunk, side, part, up)
            push(
                tok.at[chunk, side, part, up, core],
                side_land.at[chunk, axis, part],
                send,
                side_back.at[chunk, axis, 0],
                where,
            )
        add_core(chunk, 1 - sp, far, row)
        add_core(chunk, sp, near, 1 - row)
        add_core(chunk, sp, whole, row)

    def back_side(chunk):
        for axis, (part, side, up, where) in enumerate(
            ((far, 1 - sp, row, x_device), (near, sp, 1 - row, y_device))
        ):
            settle(diag_land.at[chunk, part], diag_back.at[chunk, axis])
            add(chunk, side, part, up, diag_land[chunk, part])
            push(
                tok.at[chunk, side, part, up, core],
                side_land.at[chunk, axis, part],
                send_back.at[chunk, 2],
                side_back.at[chunk, axis, 1],
                where,
            )

    def back_line(chunk):
        for axis in range(2):
            for number in range(2):
                settle(side_land.at[chunk, axis, :half], side_back.at[chunk, axis, number])
        own_sum[chunk] = tok[chunk, sp, line, row, core].astype(jnp.float32) + (
            side_land[chunk, 0, line].astype(jnp.float32)
            + side_land[chunk, 1, line].astype(jnp.float32)
        )
        add(
            chunk,
            sp,
            whole,
            row,
            side_land[chunk, 0].astype(jnp.float32) + side_land[chunk, 1].astype(jnp.float32),
        )
        for m in range(lines - 1, 0, -1):
            push(
                tok.at[chunk, sp, at_line[m], row, core],
                line_land.at[chunk, m - 1],
                send_back.at[chunk, 3],
                line_back.at[chunk, m - 1],
                line_device[m],
            )

    def close(chunk):
        total = own_sum[chunk]
        for m in range(1, lines):
            settle(line_land.at[chunk, m - 1], line_back.at[chunk, m - 1])
            total = total + line_land[chunk, m - 1].astype(jnp.float32)
        part = slice(chunk * width, (chunk + 1) * width)
        out_ref[:, part] = total

    stages = (back_diag, back_side, back_line, close)
    for step in range(chunks + len(stages)):
        if step < chunks:
            lower(step)
            meet_core(step)
        for number, stage in enumerate(stages):
            chunk = step - 1 - number
            if 0 <= chunk < chunks:
                stage(chunk)
    for chunk in range(chunks):
        settle(core_land.at[chunk], send_back.at[chunk, 0])
        settle(core_land.at[chunk, 0], send_back.at[chunk, 1])
        settle(diag_land.at[chunk], send_back.at[chunk, 2])
        settle(line_land.at[chunk], send_back.at[chunk, 3])


def layer_kernel(pitch, names, attention_count, *refs):
    table = dict(zip(names, refs))
    refs = refs[len(names) :]
    gate_ref, up_ref, down_ref, out_ref, middle_ref = refs[:5]
    refs = refs[5:]
    normed, codes, latents, weights, residual = refs[:5]
    refs = refs[5:]
    held = [name for name in names if name not in PLACED]
    inputs = dict(zip(held, refs))
    refs = refs[len(held) :]
    load_sem, gate_buf, up_buf, weight_sem = refs[:4]
    refs = refs[4:]
    attention_refs, mixture_refs = refs[:attention_count], refs[attention_count:]
    rows = normed.shape[0]
    first_width = table["out_first"].shape[0]
    own_rows = pl.ds(pl.multiple_of(lax.axis_index("tp") * rows, rows), rows)
    width = gate_buf.shape[2]

    def load(number, name):
        source = table[name]
        if name == "latent":
            target = latents.at[0]
        elif name == "out_first":
            target = weights.at[:first_width, :]
        elif name == "out_second":
            target = weights.at[first_width:, :]
        elif name == "residual":
            source, target = source.at[own_rows, :], residual
        else:
            target = inputs[name]
        return pltpu.make_async_copy(source, target, load_sem.at[number])

    loads = {name: load(number, name) for number, name in enumerate(names)}

    def weight_copies(step):
        part = pl.ds(step * width, width)
        slot = step % 2
        return (
            pltpu.make_async_copy(
                gate_ref.at[:, part, :], gate_buf.at[slot], weight_sem.at[slot, 0]
            ),
            pltpu.make_async_copy(up_ref.at[:, part, :], up_buf.at[slot], weight_sem.at[slot, 1]),
        )

    for copy in loads.values():
        copy.start()
    for step in range(2):
        for copy in weight_copies(step):
            copy.start()
    ready = [inputs[name] for name in held]
    (rotaries, queries, state, numerator, *rest) = attention_refs
    attention_kernel(
        pitch,
        *ready,
        loads,
        middle_ref,
        normed,
        codes,
        latents,
        rotaries,
        queries,
        weights,
        residual,
        state,
        numerator,
        *rest,
    )
    tok, hot, hot_turned, scale, picked, gate_sum, up_sum, active, *more = mixture_refs
    mixture_kernel(
        pitch,
        weight_copies,
        normed,
        codes,
        down_ref,
        out_ref,
        tok,
        hot,
        hot_turned,
        scale,
        picked,
        gate_sum,
        up_sum,
        active,
        gate_buf,
        up_buf,
        *more,
    )


PLACED = ("latent", "out_first", "out_second", "residual")
HELD = (
    "table",
    "first",
    "second",
    "rotary",
    "latent_gain",
    "key_first",
    "value_first",
    "key_second",
    "value_second",
    "expert_gain",
    "routes",
    "scores",
)


def run_layer(named, gate_weight, up_weight, down_weight, rows, pitch, collective_id):
    groups, sets = lax.axis_size("sp"), lax.axis_size("tp")
    lines = sets // 4
    seq_rows, rank = named["latent"].shape
    experts, depth, units = gate_weight.shape
    width, joint = depth // CHUNKS, depth // JOINT
    strip = depth // STRIPS
    first, second, rotary = named["first"], named["second"], named["rotary"]
    heads = named["out_first"].shape[0] + named["out_second"].shape[0]
    tiles = groups * sets * rows // TILE_TOKENS
    span = experts * pitch
    slots = tiles * pitch
    narrow, wide = jnp.bfloat16, jnp.float32
    anywhere = pl.BlockSpec(memory_space=pl.ANY)
    dma, keep = pltpu.SemaphoreType.DMA, pltpu.VMEM
    attention = [
        keep(rotary.shape, narrow),
        keep((first.shape[0] + second.shape[0], seq_rows), narrow),
        keep((8, seq_rows), wide),
        keep((heads, seq_rows), wide),
        keep((STRIPS, lines, 2, 2, rows, strip), narrow),
        keep((STRIPS, lines, 2, rows, strip), narrow),
        keep((STRIPS, lines, rows, strip), narrow),
        keep((STRIPS, lines - 1, rows, strip), narrow),
        keep((STRIPS, rows, strip), wide),
        dma((3 + 2 * PIECES,)),
        dma((3,)),
        dma((STRIPS,)),
        dma((STRIPS,)),
        dma((STRIPS, lines - 1)),
        dma((STRIPS, 3)),
    ]
    mixture = [
        keep((CHUNKS, groups, lines, 2, 2, rows, width), narrow),
        keep((tiles, span, TILE_TOKENS), narrow),
        keep((tiles, TILE_TOKENS, span), narrow),
        keep((experts, slots, 1), wide),
        keep((experts, slots, joint), narrow),
        keep((experts, slots, units), wide),
        keep((experts, slots, units), wide),
        keep((experts, slots, units), narrow),
        keep((CHUNKS, experts, units, width), narrow),
        keep((CHUNKS, groups, lines, 2, rows, width), narrow),
        keep((CHUNKS, lines, rows, width), narrow),
        keep((CHUNKS, 2, lines, rows, width), narrow),
        keep((CHUNKS, lines - 1, rows, width), narrow),
        keep((CHUNKS, rows, width), wide),
        dma((CHUNKS, lines - 1)),
        dma((CHUNKS, 2, lines // 2 + 1)),
        dma((CHUNKS, 2)),
        dma((CHUNKS, 4)),
        dma((CHUNKS, 4)),
        dma((CHUNKS,)),
        dma((CHUNKS, 2)),
        dma((CHUNKS, 2, 2)),
        dma((CHUNKS, lines - 1)),
        dma((CHUNKS, 4)),
        dma((CHUNKS,)),
    ]
    names = HELD + PLACED
    shared = [
        keep((rows, depth), narrow),
        keep((groups, 8, seq_rows), wide),
        keep((2, seq_rows, rank), narrow),
        keep((heads, depth), narrow),
        keep((rows, depth), narrow),
        *[keep(named[name].shape, named[name].dtype) for name in HELD],
        dma((len(names),)),
        keep((2, experts, joint, units), narrow),
        keep((2, experts, joint, units), narrow),
        dma((2, 2)),
    ]
    return pl.pallas_call(
        functools.partial(layer_kernel, pitch, names, len(attention)),
        out_shape=(
            jax.ShapeDtypeStruct((rows, depth), wide),
            jax.ShapeDtypeStruct((rows, depth), narrow),
        ),
        in_specs=[anywhere] * (len(names) + 3),
        out_specs=(VMEM, VMEM),
        scratch_shapes=shared + attention + mixture,
        compiler_params=pltpu.CompilerParams(
            collective_id=collective_id, has_side_effects=True, vmem_limit_bytes=63 << 20
        ),
        name="run_layer",
    )(*[named[name] for name in names], gate_weight, up_weight, down_weight)


def token_body(
    query_first,
    query_second,
    latent,
    key_rotary,
    latent_gain,
    key_up_first,
    value_up_first,
    key_up_second,
    value_up_second,
    out_first,
    out_second,
    residual,
    expert_gain,
    route_experts,
    route_scores,
    gate_weight,
    up_weight,
    down_weight,
):
    seq_rows = latent.shape[0]
    sets = lax.axis_size("tp")
    groups = lax.axis_size("sp")
    own_rows = seq_rows // sets
    span_blocks = TILE_TOKENS // own_rows
    pitch = -(-span_blocks * CAP // 16) * 16
    half = key_rotary.shape[1] // 2
    inverse = np.float32(rotary_base) ** (-np.arange(half, dtype=np.float32) / half)
    angles = inverse[:, None] * np.arange(groups * seq_rows, dtype=np.float32)[None, :]
    table = np.concatenate([np.cos(angles), np.sin(angles)], axis=0).astype(np.float32)
    named = {
        "table": jnp.asarray(table),
        "first": query_first.T,
        "second": query_second.T,
        "latent": latent,
        "rotary": key_rotary.T,
        "latent_gain": latent_gain[None, :],
        "key_first": key_up_first.T,
        "value_first": value_up_first.T,
        "key_second": key_up_second,
        "value_second": value_up_second,
        "out_first": out_first,
        "out_second": out_second,
        "residual": residual,
        "expert_gain": expert_gain[None, :],
        "routes": route_experts.T,
        "scores": route_scores.T,
    }
    mixture, middle = run_layer(
        named, gate_weight, up_weight, down_weight, own_rows, pitch, 0
    )
    return (middle.astype(jnp.float32) + mixture).astype(jnp.bfloat16)


def solution(mesh):
    in_specs = (
        P("sp", "tp"),
        P("sp", "tp"),
        P("sp", None),
        P("sp", None),
        P(),
        P(None, "tp"),
        P(None, "tp"),
        P(None, "tp"),
        P(None, "tp"),
        P("tp", None),
        P("tp", None),
        P("sp", None),
        P(),
        P("sp", None),
        P("sp", None),
        P("sp", None, "tp"),
        P("sp", None, "tp"),
        P("sp", "tp", None),
    )
    out_specs = P(("sp", "tp"), None)
    groups, sets = mesh.shape["sp"], mesh.shape["tp"]
    small = groups == 2 and sets & (sets - 1) == 0 and sets > 4

    def body(*arguments):
        fits = small and arguments[2].shape[0] * groups <= 1024
        return (token_body if fits else slot_body)(*arguments)

    return jax.shard_map(body, mesh=mesh, in_specs=in_specs, out_specs=out_specs, check_vma=False)
```
